512 devices in a mesh: sp: 256 (over z, y, x), tp: 2 (over core).
Axes of the slice: x: 4, y: 8, z: 8, core: 2. Of those that a mesh axis runs over, the one named last changes fastest.
Arguments:
- tokens: bfloat16 [32768, 2048], P('sp', 'tp'), may hold values from -6 to 6
- in_gain: bfloat16 [1, 2048], P(None, 'tp'), may hold values from 0.099609375 to 1.8984375
- w_input: bfloat16 [2048, 1024], P(None, 'tp'), may hold values from -0.125 to 0.125
- w_bgate: bfloat16 [2048, 1024], P(None, 'tp'), may hold values from -0.125 to 0.125
- w_cgate: bfloat16 [2048, 1024], P(None, 'tp'), may hold values from -0.125 to 0.125
- w_value: bfloat16 [2048, 1024], P(None, 'tp'), may hold values from -0.125 to 0.125
- decay_rate: float32 [64, 64], P('tp'), may hold values from 6.1035156e-06 to 0.034, as said below
- angle: float32 [64, 64], P('tp'), may hold values from -3.140625 to 3.140625
- decay_shift: float32 [64, 32768], P('tp', 'sp'), may hold values from -1.1 to 0, as said below
- b_input: float32 [2, 64, 64, 16], P(None, 'tp'), may hold values from -1 to 1
- c_output: float32 [2, 64, 16, 64], P(None, 'tp'), may hold values from -0.75 to 0.75
- initial_recurrence_vector: float32 [2, 64, 64], P(None, 'tp'), may hold values from -1086.116 to 1086.116
- skip_gain: float32 [1024], P('tp'), may hold values from -4 to 4
- ssm_gain: float32 [1024], P('tp'), may hold values from 0.1 to 1.9
- conv_gain: float32 [1024], P('tp'), may hold values from 0.1 to 1.9
- conv_taps: float32 [3, 1024], P(None, 'tp'), may hold values from -3.5 to 3.5
- w_out_ssm: bfloat16 [1024, 2048], P('tp'), may hold values from -0.125 to 0.125
- w_out_conv: bfloat16 [1024, 2048], P('tp'), may hold values from -0.125 to 0.125
Outputs:
- mixed: bfloat16 [32768, 2048], P(('sp', 'tp'))
The draws below stay inside these ranges and needn't reach their ends.
Inputs may be any that keep to these rules, and one draw needn't show every extreme that they name: `decay_rate`: positive rates. `decay_shift`: never positive.
All inputs are finite; a program needn't handle non-finite values.
Results may differ from the reference program's by a relative error of at most 0.0085.
Values may be sent and summed in bfloat16 or wider, within the bound.
A program may use at most 64 MiB of HBM per device.

```python
import math
import jax
import jax.numpy as jnp
from jax import lax

D = 2048
SSM_GROUPS = 64
GROUP_CH = 16
STATE = 64
CONVOLUTION_CHAN = 64
KERNEL = 3
TOK_DEV = 128
TOKENS = 32768
D_SSM = 1024
D_CONV = 1024
N_TP = 2


def slow_groups(key):
    share = 0.5
    return jax.random.uniform(jax.random.fold_in(key, 11), (SSM_GROUPS,), jnp.float32) < share


def draw_decay_rate(key, part):
    slow = slow_groups(key)
    spread = jax.random.uniform(jax.random.fold_in(key, 12), (SSM_GROUPS, STATE), jnp.float32)
    slow_rate = (0.2 + 0.3 * spread) / TOKENS
    fast_rate = jnp.exp(math.log(0.01) + spread * (math.log(1.0 / 30.0) - math.log(0.01)))
    return jnp.where(slow[:, None], slow_rate, fast_rate).astype(jnp.float32)


def draw_decay_shift(key, part):
    slow = slow_groups(key)
    factor = jax.random.uniform(jax.random.fold_in(key, 13), (SSM_GROUPS, TOKENS // TOK_DEV), jnp.float32)
    level = jnp.where(slow, 0.5 / TOKENS, 1.0 / 60.0)
    starting_shift_amount = -jnp.repeat(factor * level[:, None], TOK_DEV, axis=1)
    slot_numbers_list = jax.random.randint(jax.random.fold_in(key, 14), (SSM_GROUPS, 2), 0, TOKENS)
    objective_errors = jax.random.uniform(jax.random.fold_in(key, 15), (SSM_GROUPS, 2), jnp.float32, 0.2, 0.4)
    sequence_slot_number = jnp.arange(TOKENS)[None, :]
    symbol_batches_count = jnp.where(sequence_slot_number == slot_numbers_list[:, 0:1], jnp.log(1.0 - objective_errors[:, 0:1]), 0.0)
    symbol_batches_count = symbol_batches_count + jnp.where(sequence_slot_number == slot_numbers_list[:, 1:2], jnp.log(1.0 - objective_errors[:, 1:2]), 0.0)
    return (starting_shift_amount + symbol_batches_count).astype(jnp.float32)


def steps_of(own_key, dims, cuts, smallest, largest):
    level, own = 1.0, jax.random.fold_in(own_key, 6)
    for position, shards_of in cuts:
        draws = jnp.exp(jax.random.uniform(jax.random.fold_in(own, position), (shards_of,), jnp.float32, smallest / len(cuts), largest / len(cuts)))
        level = level * jnp.repeat(draws, dims[position] // shards_of).reshape([-1 if axis == position else 1 for axis in range(len(dims))])
    return level


def noise(rng, dims, scale, limit, cuts=(), held_as=jnp.bfloat16):
    loudness = steps_of(rng, dims, cuts, -0.22, 0.18) if cuts else 1.0
    drawn = jax.random.normal(rng, dims, jnp.float32) * scale * loudness
    return jnp.minimum(jnp.maximum(drawn, -limit), limit).astype(held_as)


def setup_inputs(seed: int = 0) -> dict:
    streams_of = jax.random.split(jax.random.key(seed), 19)
    return {
        "tokens": noise(streams_of[0], (TOKENS, D), 1.0, 6.0, ((0, 256), (1, 2))),
        "in_gain": jnp.clip(1.0 + 0.18 * jax.random.normal(streams_of[1], (1, D), jnp.float32), 0.099609375, 1.8984375).astype(jnp.bfloat16),
        "w_input": noise(streams_of[2], (D, D_SSM), D ** -0.5, 0.125, ((1, 2),)),
        "w_bgate": noise(streams_of[3], (D, D_CONV), D ** -0.5, 0.125, ((1, 2),)),
        "w_cgate": noise(streams_of[4], (D, D_CONV), D ** -0.5, 0.125, ((1, 2),)),
        "w_value": noise(streams_of[5], (D, D_CONV), D ** -0.5, 0.125, ((1, 2),)),
        "decay_rate": draw_decay_rate(jax.random.fold_in(streams_of[18], 71), 0),
        "angle": jnp.clip(jax.random.uniform(streams_of[7], (SSM_GROUPS, STATE), jnp.float32, -3.140625, 3.140625), -3.140625, 3.140625),
        "decay_shift": draw_decay_shift(jax.random.fold_in(streams_of[18], 71), 0),
        "b_input": noise(streams_of[9], (2, SSM_GROUPS, STATE, GROUP_CH), (2 * GROUP_CH) ** -0.5, 1.0, ((1, 2),), jnp.float32),
        "c_output": noise(streams_of[10], (2, SSM_GROUPS, GROUP_CH, STATE), STATE ** -0.5, 0.75, ((1, 2),), jnp.float32),
        "initial_recurrence_vector": noise(streams_of[11], (2, SSM_GROUPS, STATE), (TOKENS ** 0.5), 1086.116, ((1, 2),), jnp.float32),
        "skip_gain": noise(streams_of[12], (D_SSM,), 1.0, 4.0, ((0, 2),), jnp.float32),
        "ssm_gain": jnp.clip(1.0 + 0.18 * jax.random.normal(streams_of[13], (D_SSM,), jnp.float32), 0.1, 1.9),
        "conv_gain": jnp.clip(1.0 + 0.18 * jax.random.normal(streams_of[14], (D_CONV,), jnp.float32), 0.1, 1.9),
        "conv_taps": noise(streams_of[15], (KERNEL, D_CONV), KERNEL ** -0.5, 3.5, ((1, 2),), jnp.float32),
        "w_out_ssm": noise(streams_of[16], (D_SSM, D), (D_SSM + D_CONV) ** -0.5, 0.125, ((0, 2),)),
        "w_out_conv": noise(streams_of[17], (D_CONV, D), (D_SSM + D_CONV) ** -0.5, 0.125, ((0, 2),)),
    }


def complex_step(first, second):
    ar1, ai1, br1, bi1 = first
    ar2, ai2, br2, bi2 = second
    return (ar2 * ar1 - ai2 * ai1, ar2 * ai1 + ai2 * ar1, ar2 * br1 - ai2 * bi1 + br2, ar2 * bi1 + ai2 * br1 + bi2)

def input_matrix(decay_rate, angle, b_input):
    real_part = jnp.expm1(-decay_rate) * jnp.cos(angle) - 2.0 * jnp.sin(0.5 * angle) ** 2
    imag_part = jnp.exp(-decay_rate) * jnp.sin(angle)
    denom = decay_rate * decay_rate + angle * angle
    zoh_re = (imag_part * angle - real_part * decay_rate) / denom
    zoh_im = -(imag_part * decay_rate + real_part * angle) / denom
    b_re = zoh_re[..., None] * b_input[0] - zoh_im[..., None] * b_input[1]
    b_im = zoh_re[..., None] * b_input[1] + zoh_im[..., None] * b_input[0]
    return (b_re, b_im)

def head_norm(values, gain, width):
    count, total = values.shape
    grouped = values.reshape(count, total // width, width)
    grouped = grouped * lax.rsqrt(lax.optimization_barrier(jnp.mean(grouped * grouped, axis=-1, keepdims=True)) + 1e-06)
    return (grouped.reshape(count, total) * gain).astype(jnp.bfloat16)

def reference(tokens, in_gain, w_input, w_bgate, w_cgate, w_value, decay_rate, angle, decay_shift, b_input, c_output, initial_recurrence_vector, skip_gain, ssm_gain, conv_gain, conv_taps, w_out_ssm, w_out_conv):
    highest = lax.Precision.HIGHEST
    floats = tokens.astype(jnp.float32)
    inv = lax.rsqrt(lax.optimization_barrier(jnp.mean(floats * floats, axis=-1, keepdims=True)) + 1e-06)
    scaled = (floats * in_gain[0].astype(jnp.float32)).astype(jnp.bfloat16)
    u_in = (jnp.dot(scaled, w_input, preferred_element_type=jnp.float32) * inv).astype(jnp.bfloat16)
    bgate = (jnp.dot(scaled, w_bgate, preferred_element_type=jnp.float32) * inv).astype(jnp.bfloat16)
    cgate = (jnp.dot(scaled, w_cgate, preferred_element_type=jnp.float32) * inv).astype(jnp.bfloat16)
    value = (jnp.dot(scaled, w_value, preferred_element_type=jnp.float32) * inv).astype(jnp.bfloat16)
    b_re, b_im = input_matrix(decay_rate, angle, b_input)
    u_groups = u_in.astype(jnp.float32).reshape(TOKENS, SSM_GROUPS, GROUP_CH).transpose(1, 0, 2)

    def single_group(items):
        u_grp, rate, theta, shift, bre, bim, c_re, c_im, init_re, init_im = items
        drive_re = jnp.dot(u_grp, bre.T, precision=highest)
        drive_im = jnp.dot(u_grp, bim.T, precision=highest)
        magnitude = jnp.exp(shift[:, None] - rate[None, :])
        step_re = magnitude * jnp.cos(theta)[None, :]
        step_im = magnitude * jnp.sin(theta)[None, :]
        cum = lax.associative_scan(complex_step, (step_re, step_im, drive_re, drive_im), axis=0)
        state_re = cum[2] + cum[0] * init_re[None, :] - cum[1] * init_im[None, :]
        state_im = cum[3] + cum[0] * init_im[None, :] + cum[1] * init_re[None, :]
        return jnp.dot(state_re, c_re.T, precision=highest) - jnp.dot(state_im, c_im.T, precision=highest)
    outputs = lax.map(single_group, (u_groups, decay_rate, angle, decay_shift, b_re, b_im, c_output[0], c_output[1], initial_recurrence_vector[0], initial_recurrence_vector[1]))
    ssm_pre = outputs.transpose(1, 0, 2).reshape(TOKENS, D_SSM) + skip_gain * u_in.astype(jnp.float32)
    state_space_output = head_norm(jax.nn.gelu(ssm_pre, approximate=False), ssm_gain, GROUP_CH)
    gated = cgate.astype(jnp.float32) * value.astype(jnp.float32)
    padded = jnp.concatenate([jnp.zeros((KERNEL - 1, D_CONV), jnp.float32), gated], axis=0)
    conv = padded[0:TOKENS] * conv_taps[0]
    for tap in range(1, KERNEL):
        conv = conv + padded[tap:tap + TOKENS] * conv_taps[tap]
    conv_out = head_norm(bgate.astype(jnp.float32) * conv, conv_gain, CONVOLUTION_CHAN)
    ssm_width = D_SSM // N_TP
    filter_tap_length = D_CONV // N_TP
    total = jnp.zeros((TOKENS, D), jnp.float32)
    for block in range(N_TP):
        lo = block * ssm_width
        start = block * filter_tap_length
        partial_sum = jnp.dot(state_space_output[:, lo:lo + ssm_width], w_out_ssm[lo:lo + ssm_width], preferred_element_type=jnp.float32)
        partial_sum = partial_sum + jnp.dot(conv_out[:, start:start + filter_tap_length], w_out_conv[start:start + filter_tap_length], preferred_element_type=jnp.float32)
        rounded = lax.optimization_barrier(partial_sum.astype(jnp.bfloat16))
        total = total + rounded.astype(jnp.float32)
    return total.astype(jnp.bfloat16)
```

```python
import functools
import math

import jax
import jax.numpy as jnp
from jax import lax
from jax.experimental import pallas as pl
from jax.experimental.pallas import tpu as pltpu
from jax.sharding import Mesh
from jax.sharding import PartitionSpec as P

D = 2048
HALF = 1024
CH = 512
GROUPS = 32
ENTRIES = 64
ROWS = 128
PAIRS = 16
SP_DIMS = (8, 8, 4)
SP = ("sz", "sy", "sx")
F32 = jnp.float32
BF16 = jnp.bfloat16
HIGHEST = lax.Precision.HIGHEST


def cmul(a, b):
    return (a[0] * b[0] - a[1] * b[1], a[0] * b[1] + a[1] * b[0])


def cadd(a, b):
    return (a[0] + b[0], a[1] + b[1])


def expm1(v):
    series = 1.0 + v / 8.0
    for k in range(7, 1, -1):
        series = 1.0 + series * v / k
    return jnp.where(jnp.abs(v) < 0.3, v * series, jnp.exp(v) - 1.0)


def split(v):
    high = v.astype(BF16)
    return high, (v - high.astype(F32)).astype(BF16)


def iota(shape, dim):
    return lax.broadcasted_iota(jnp.int32, shape, dim)


def kernel(
    dims,
    tokens,
    in_gain,
    w_input,
    w_bgate,
    w_cgate,
    w_value,
    decay_rate,
    angle,
    decay_shift,
    b_input,
    c_output,
    initial,
    skip_gain,
    ssm_gain,
    conv_gain,
    conv_taps,
    w_out_ssm,
    w_out_conv,
    out,
    tok_v,
    gain_v,
    win_v,
    wb_v,
    wc_v,
    wv_v,
    rate_v,
    angle_v,
    shift_v,
    b_v,
    c_v,
    init_v,
    skip_v,
    sgain_v,
    cgain_v,
    taps_v,
    wos_v,
    woc_v,
    acc_v,
    u_v,
    bw_v,
    cw_v,
    ce_v,
    expf_v,
    at_v,
    bt_v,
    wneg_v,
    wpos_v,
    wposb_v,
    q_v,
    sum_v,
    mixed_v,
    ypre_v,
    pad_v,
    bg_v,
    cpart_v,
    sout_v,
    part_v,
    got_v,
    sx_v,
    sy_v,
    sz_v,
    mx_v,
    my_v,
    mz_v,
    load_sem,
    tok_sem,
    tail_sem,
    part_ss,
    part_rs,
    sx_sem,
    sy_sem,
    sz_sem,
    mx_sem,
    my_sem,
    mz_sem,
    ring2,
    ring3,
    zring2,
    zring3,
    zring4,
):
    nz, ny, nx = dims
    z, y, x = (lax.axis_index(a) for a in SP)
    tp = lax.axis_index("tp")
    other = 1 - tp
    coords = {"sz": (z, nz), "sy": (y, ny), "sx": (x, nx)}

    pairs = [
        (tokens, tok_v.at[tp]),
        (in_gain, gain_v.at[tp]),
        (w_input.at[pl.ds(tp * HALF, HALF)], win_v.at[pl.ds(tp * HALF, HALF)]),
        (decay_shift, shift_v),
        (decay_rate, rate_v),
        (angle, angle_v),
        (w_input.at[pl.ds(other * HALF, HALF)], win_v.at[pl.ds(other * HALF, HALF)]),
        (b_input, b_v),
        (w_cgate, wc_v),
        (w_value, wv_v),
        (c_output, c_v),
        (w_bgate, wb_v),
        (initial, init_v),
        (skip_gain, skip_v),
        (ssm_gain, sgain_v),
        (conv_gain, cgain_v),
        (conv_taps, taps_v),
        (w_out_conv, woc_v),
        (w_out_ssm, wos_v),
    ]
    loads = [pltpu.make_async_copy(s, d, load_sem.at[k]) for k, (s, d) in enumerate(pairs)]
    for k in (0, 1, 3, 4, 5, 2, 7, 6):
        loads[k].start()

    def near(axis):
        n = coords[axis][1]
        return [] if n == 1 else ([1] if n == 2 else [1, n - 1])

    def at_step(axis, step):
        here, n = coords[axis]
        return {axis: lax.rem(here + step, n)}

    around = [at_step(a, s) for a in ("sy", "sx") for s in near(a)]
    far = [at_step("sx", s) for s in near("sx")]
    far += [at_step("sy", s) for s in (2, 6) if ny == 8]

    def tell(sem, step, above=True):
        @pl.when(z >= step)
        def _():
            pl.semaphore_signal(sem, inc=1, device_id={"sz": z - step})

        if above:

            @pl.when(z + step < nz)
            def _():
                pl.semaphore_signal(sem, inc=1, device_id={"sz": z + step})

    def beside(step):
        return jnp.where(z + step < nz, 1, 0) + jnp.where(z >= step, 1, 0)

    barrier = pltpu.get_barrier_semaphore()
    for dev in [{"tp": other}] + around:
        pl.semaphore_signal(barrier, inc=1, device_id=dev)
    tell(barrier, 1)

    loads[0].wait()
    loads[1].wait()
    pl.semaphore_wait(barrier, 1 + len(around) + beside(1))

    tok_copy = pltpu.make_async_remote_copy(
        tok_v.at[tp], tok_v.at[tp], tok_sem.at[0], tok_sem.at[1], device_id={"tp": other}
    )
    gain_copy = pltpu.make_async_remote_copy(
        gain_v.at[tp], gain_v.at[tp], tok_sem.at[2], tok_sem.at[3], device_id={"tp": other}
    )
    tok_copy.start()
    gain_copy.start()
    for dev in around:
        pl.semaphore_signal(ring2, inc=1, device_id=dev)
    if nz > 2:
        tell(zring2, 1)
    for k in range(8, len(loads)):
        loads[k].start()

    def exchange(buf, sems, axis, later):
        here, n = coords[axis]
        order = sorted(range(1, n), key=lambda s: -min(s, n - s))

        def copy(step):
            return pltpu.make_async_remote_copy(
                buf.at[here],
                buf.at[here],
                sems.at[0, step],
                sems.at[1, step],
                device_id=at_step(axis, step),
            )

        def start():
            for s in order:
                if later:
                    pl.when(here + s < n)(copy(s).start)
                else:
                    copy(s).start()

        def incoming(step):
            slot = lax.rem(here + n - step, n)
            return pltpu.make_async_remote_copy(
                buf.at[slot],
                buf.at[slot],
                sems.at[0, step],
                sems.at[1, step],
                device_id=at_step(axis, step),
            )

        def wait_recv():
            for s in range(1, n):
                if later:
                    pl.when(here >= s)(incoming(s).wait_recv)
                else:
                    incoming(s).wait_recv()

        def wait_send():
            for s in range(1, n):
                if later:
                    pl.when(here + s < n)(copy(s).wait_send)
                else:
                    copy(s).wait_send()

        return start, wait_recv, wait_send

    sx = exchange(sx_v, sx_sem, "sx", False)
    sy = exchange(sy_v, sy_sem, "sy", False)
    sz = exchange(sz_v, sz_sem, "sz", True)
    mx = exchange(mx_v, mx_sem, "sx", False)
    my = exchange(my_v, my_sem, "sy", False)
    mz = exchange(mz_v, mz_sem, "sz", True)

    def half(which):
        floats = tok_v[which].astype(F32)
        scaled = (floats * gain_v[which].astype(F32)).astype(BF16)
        return scaled, jnp.sum(floats * floats, axis=1, keepdims=True)

    loads[3].wait()
    tri = (iota((ROWS, ROWS), 0) >= iota((ROWS, ROWS), 1)).astype(F32)
    shifts = jnp.concatenate([shift_v[...], jnp.zeros((ROWS - GROUPS, ROWS), F32)], axis=0)
    logs = lax.dot_general(
        tri, shifts, (((1,), (1,)), ((), ())), precision=HIGHEST, preferred_element_type=F32
    )
    sigma = logs[ROWS - 1 : ROWS]
    mid = logs[ROWS // 2 - 1 : ROWS // 2]
    sx_v[x] = sigma

    loads[4].wait()
    loads[5].wait()

    def paired(ref, lead=()):
        even = ref[(*lead, pl.ds(0, PAIRS, 2), slice(None))]
        odd = ref[(*lead, pl.ds(1, PAIRS, 2), slice(None))]
        return jnp.concatenate([even, odd], axis=1)

    rate = paired(rate_v)
    theta = paired(angle_v)

    def power(k):
        mag = jnp.exp(-rate * float(k))
        ph = theta * float(k)
        return (mag * jnp.cos(ph), mag * jnp.sin(ph))

    cos1, sin1 = jnp.cos(theta), jnp.sin(theta)
    unit = (cos1, sin1)
    lane = iota((1, ROWS), 1)
    grp = iota((PAIRS, ROWS), 0)
    grp_lane = iota((PAIRS, ROWS), 1)
    spread_h = (
        (iota((ROWS, ROWS), 0) % 2 == iota((ROWS, ROWS), 1) // ENTRIES)
        & (iota((ROWS, ROWS), 0) < GROUPS)
    ).astype(F32)

    def expand(rows):
        blocks = [jnp.where(grp_lane // 2 == grp, row, 0.0) for row in rows]
        wide = jnp.dot(
            jnp.concatenate(blocks, axis=0), spread_h, precision=HIGHEST, preferred_element_type=F32
        )
        return [wide[PAIRS * k : PAIRS * (k + 1)] for k in range(len(rows))]

    keep = lane < GROUPS
    ratio = jnp.concatenate([jnp.exp(mid - logs), jnp.exp(logs - mid)], axis=0)
    ratio = jnp.where(keep, ratio, 0.0)
    hi = ratio.astype(BF16)
    lo = ratio - hi.astype(F32)
    both = hi.astype(F32) + pltpu.roll(lo, GROUPS, 1)
    both = both.astype(BF16)
    mixed_v[...] = both

    def spread(part):
        for k in range(PAIRS // 2):
            src = iota((ROWS, 256), 0)
            dst = iota((ROWS, 256), 1) + 256 * k
            pick = ((src % GROUPS == dst // ENTRIES) & (src < 2 * GROUPS)).astype(F32).astype(BF16)
            wide = jnp.dot(
                mixed_v[ROWS * part : ROWS * (part + 1), :], pick, preferred_element_type=F32
            )
            expf_v[part, 2 * k] = wide[:, :ROWS]
            expf_v[part, 2 * k + 1] = wide[:, ROWS:]

    spread(0)

    ph = unit
    for b in range(8):
        bt_v[0, pl.ds(b, PAIRS, 8), :] = ph[0]
        bt_v[1, pl.ds(b, PAIRS, 8), :] = ph[1]
        mag = jnp.exp(-rate * float(b + 1))
        bt_v[2, pl.ds(b, PAIRS, 8), :] = mag
        bt_v[3, pl.ds(b, PAIRS, 8), :] = 1.0 / mag
        ph8 = ph
        ph = cmul(ph, unit)
    ph = (jnp.ones_like(cos1), jnp.zeros_like(cos1))
    for a in range(8, 16):
        at_v[0, a], at_v[1, a] = ph
        mag = jnp.exp(-rate * float(8 * (a - 8)))
        at_v[2, a], at_v[3, a] = mag, 1.0 / mag
        ph = cmul(ph, ph8)
        back = 16 - (a + 1)
        at_v[0, back], at_v[1, back] = ph[0], -ph[1]
        mag = jnp.exp(rate * float(8 * (8 - back)))
        at_v[2, back], at_v[3, back] = mag, 1.0 / mag

    def table(part, store):
        @pl.loop(0, PAIRS)
        def _(r):
            cb, sb, mb = (bt_v[k, pl.ds(r * 8, 8), :] for k in (0, 1, 3 - part))
            for a in range(16):
                ca, sa, ma = (
                    jnp.broadcast_to(at_v[k, a, pl.ds(r, 1), :], (8, ROWS)) for k in (0, 1, 3 - part)
                )
                c, s = cmul((ca, sa), (cb, sb))
                span = slice(8 * a, 8 * a + 8)
                store(r, span, c, s, ma * mb * expf_v[part, r, span, :])

    def backward(r, span, c, s, scale):
        wneg_v[0, r, span, :] = c * scale
        wneg_v[1, r, span, :] = -s * scale

    def forward(r, span, c, s, scale):
        wpos_v[0, r, span, :] = c * scale
        wpos_v[1, r, span, :] = s * scale

    table(0, backward)
    mid_wide, rest_wide = expand([mid, sigma - mid])
    p64 = power(64)
    end = cmul((at_v[0, 15], at_v[1, 15]), ph8)
    fall = jnp.exp(rest_wide) * jnp.exp(-rate * 64.0)
    last = (end[0] * fall, end[1] * fall)
    enter = (p64[0] * jnp.exp(mid_wide), p64[1] * jnp.exp(mid_wide))

    loads[7].wait()
    dec = expm1(-rate) * cos1 - 2.0 * jnp.sin(0.5 * theta) ** 2
    ims = jnp.exp(-rate) * sin1
    den = rate * rate + theta * theta
    zr = (ims * theta - dec * rate) / den
    zi = -(ims * rate + dec * theta) / den
    sum_v[0], sum_v[1] = zr, zi
    mask = iota((32, ROWS), 0) // 16 == iota((32, ROWS), 1) // ENTRIES
    for r in range(PAIRS):
        span = slice(32 * r, 32 * r + 32)
        br, bi = b_v[0, span, :], b_v[1, span, :]
        br = jnp.concatenate([br, br], axis=1)
        bi = jnp.concatenate([bi, bi], axis=1)
        wr, wi = cmul((sum_v[0, r : r + 1, :], sum_v[1, r : r + 1, :]), (br, bi))
        at = 32 * (r % 4)
        for k, w in enumerate((wr, wi)):
            lanes = slice(ROWS * k, ROWS * (k + 1))
            high, low = split(jnp.where(mask, w, 0.0))
            bw_v[r // 4, at : at + 32, lanes] = high
            bw_v[r // 4, ROWS + at : ROWS + at + 32, lanes] = low

    own_scaled, own_sq = half(tp)
    loads[2].wait()
    acc_v[...] = jnp.dot(
        own_scaled, win_v[pl.ds(tp * HALF, HALF), :], preferred_element_type=F32
    )

    if around:
        pl.semaphore_wait(ring2, len(around))
    sx[0]()
    for dev in far:
        pl.semaphore_signal(ring3, inc=1, device_id=dev)
    if nz > 2:
        pl.semaphore_wait(zring2, beside(1))
        tell(zring3, 2)

    tok_copy.wait_recv()
    gain_copy.wait_recv()
    far_scaled, far_sq = half(other)
    inv = lax.rsqrt((own_sq + far_sq) / D + 1e-06)
    loads[6].wait()
    acc = acc_v[...] + jnp.dot(
        far_scaled, win_v[pl.ds(other * HALF, HALF), :], preferred_element_type=F32
    )
    u_v[...] = (acc * inv).astype(BF16)

    quarter = iota((ROWS, ROWS), 1) // 32
    for j in range(4):
        uj = u_v[:, ROWS * j : ROWS * (j + 1)]
        stacked = jnp.concatenate(
            [jnp.where(quarter == i, uj, jnp.zeros_like(uj)) for i in range(4)], axis=0
        )
        drive = jnp.dot(
            jnp.concatenate([stacked, stacked], axis=1), bw_v[j], preferred_element_type=F32
        )
        for i in range(4):
            r = 4 * j + i
            d = drive[ROWS * i : ROWS * (i + 1)]
            q = cmul((wneg_v[0, r], wneg_v[1, r]), (d[:, :ROWS], d[:, ROWS:]))
            sum_v[0, r : r + 1, :] = jnp.sum(q[0], axis=0, keepdims=True)
            sum_v[1, r : r + 1, :] = jnp.sum(q[1], axis=0, keepdims=True)
            q_v[r, :, 0:ROWS] = q[0]
            q_v[r, :, ROWS:] = q[1]
    mine = cmul(last, (sum_v[0], sum_v[1]))

    def put(buf, index, value):
        buf[index, 0:PAIRS, :] = value[0]
        buf[index, PAIRS : 2 * PAIRS, :] = value[1]

    def take(buf, index):
        return (buf[index, 0:PAIRS, :], buf[index, PAIRS : 2 * PAIRS, :])

    put(mx_v, x, mine)
    mx[0]()

    sx[1]()
    rows = [sx_v[k] for k in range(nx)]
    rho = functools.reduce(jnp.add, rows)
    sy_v[y] = rho
    if far:
        pl.semaphore_wait(ring3, len(far))
    sy[0]()
    wide = expand(rows)
    p128 = power(ROWS)
    ax = [(p128[0] * jnp.exp(w), p128[1] * jnp.exp(w)) for w in wide]

    def sweep(steps, values, start, here):
        total = before = start
        for k in range(len(steps)):
            if k:
                before = tuple(jnp.where(here == k, t, b) for t, b in zip(total, before))
            total = cmul(steps[k], total)
            if values is not None:
                total = cadd(total, values[k])
        return before, total

    one = (jnp.ones_like(cos1), jnp.zeros_like(cos1))
    zero = (jnp.zeros_like(cos1), jnp.zeros_like(cos1))
    dx, _ = sweep(ax, None, one, x)

    def project(w):
        acc = jnp.dot(own_scaled, w[pl.ds(tp * HALF, HALF), :], preferred_element_type=F32)
        acc = acc + jnp.dot(far_scaled, w[pl.ds(other * HALF, HALF), :], preferred_element_type=F32)
        return (acc * inv).astype(BF16).astype(F32)

    loads[8].wait()
    loads[9].wait()
    pad_v[8:, :] = project(wc_v) * project(wv_v)
    index = (z * ny + y) * nx + x
    count = nz * ny * nx
    x1 = lax.rem(x + 1, nx)
    carry = x + 1 == nx
    y1 = jnp.where(carry, lax.rem(y + 1, ny), y)
    z1 = jnp.where(carry & (y + 1 == ny), lax.rem(z + 1, nz), z)
    tail_copy = pltpu.make_async_remote_copy(
        pad_v.at[ROWS : ROWS + 8],
        pad_v.at[0:8],
        tail_sem.at[0],
        tail_sem.at[1],
        device_id={"sz": z1, "sy": y1, "sx": x1},
    )
    pl.when(index + 1 < count)(tail_copy.start)

    spread(1)
    table(1, forward)
    if nz > 2:

        @pl.when(beside(2) > 0)
        def _():
            pl.semaphore_wait(zring3, beside(2))

    if nz > 4:
        tell(zring4, 4, above=False)

    mx[1]()
    pre_x, row_total = sweep(ax, [take(mx_v, k) for k in range(nx)], zero, x)
    put(my_v, y, row_total)
    my[0]()

    sy[1]()
    rows = [sy_v[k] for k in range(ny)]
    pi = functools.reduce(jnp.add, rows)
    sz_v[z] = pi
    if nz > 4:

        @pl.when(z + 4 < nz)
        def _():
            pl.semaphore_wait(zring4, 1)

    sz[0]()
    p512 = power(ROWS * nx)
    ay = [(p512[0] * jnp.exp(w), p512[1] * jnp.exp(w)) for w in expand(rows)]
    dy, _ = sweep(ay, None, one, y)
    pz = power(ROWS * nx * ny)

    loads[10].wait()
    for r in range(PAIRS):
        span = slice(32 * r, 32 * r + 32)
        cr, ci = c_v[0, span, :], c_v[1, span, :]
        cw_v[span, 0:ROWS] = jnp.where(mask, jnp.concatenate([cr, cr], axis=1), 0.0)
        cw_v[span, ROWS:] = jnp.where(mask, jnp.concatenate([ci, ci], axis=1), 0.0)
    tri16 = jnp.concatenate([tri.astype(BF16), tri.astype(BF16)], axis=1)
    sign = jnp.where(iota((1, 256), 1) < ROWS, 1.0, -1.0)
    nt = (((1,), (1,)), ((), ()))

    def gathered(wide):
        total = jnp.where(quarter == 0, wide[0:ROWS], 0.0)
        for i in range(1, 4):
            total = jnp.where(quarter == i, wide[ROWS * i : ROWS * (i + 1)], total)
        return total

    def read_out(high, low, weights):
        wide = lax.dot_general(high, weights, nt, preferred_element_type=F32)
        rest = lax.dot_general(low, weights[0:ROWS], nt, preferred_element_type=F32)
        return gathered(wide[:, :ROWS] + wide[:, ROWS:] + rest)

    loads[13].wait()
    for j in range(4):
        highs, lows = [], []
        for i in range(4):
            r = 4 * j + i
            pre = jnp.dot(
                tri16, jnp.concatenate(split(q_v[r]), axis=0), preferred_element_type=F32
            )
            st = cmul((wpos_v[0, r], wpos_v[1, r]), (pre[:, :ROWS], pre[:, ROWS:]))
            high, low = zip(*(split(part) for part in st))
            highs.append(jnp.concatenate(high, axis=1))
            lows.append(jnp.concatenate(low, axis=1))
            for k in range(2):
                lanes = slice(ROWS * k, ROWS * (k + 1))
                span = slice(ROWS * r, ROWS * (r + 1))
                wposb_v[0, span, lanes], wposb_v[1, span, lanes] = split(wpos_v[k, r])
        cols = slice(ROWS * j, ROWS * (j + 1))
        weights = jnp.concatenate(split(cw_v[cols, :] * sign), axis=0)
        read = read_out(jnp.concatenate(highs, axis=0), jnp.concatenate(lows, axis=0), weights)
        ypre_v[:, cols] = read + skip_v[:, cols] * u_v[:, cols].astype(F32)

    my[1]()
    pre_y, plane_total = sweep(ay, [take(my_v, k) for k in range(ny)], zero, y)
    put(mz_v, z, plane_total)
    mz[0]()

    loads[11].wait()
    bg_v[...] = project(wb_v)

    @pl.when(index == 0)
    def _():
        pad_v[0:8, :] = jnp.zeros((8, CH), F32)

    pl.when(index > 0)(tail_copy.wait_recv)
    loads[15].wait()
    loads[16].wait()
    conv = pad_v[6 : 6 + ROWS, :] * taps_v[0:1, :]
    conv = conv + pad_v[7 : 7 + ROWS, :] * taps_v[1:2, :]
    conv = conv + pad_v[8 : 8 + ROWS, :] * taps_v[2:3, :]

    def head_norm(values, gain, width):
        same = iota((ROWS, ROWS), 0) // width == iota((ROWS, ROWS), 1) // width
        mean = jnp.where(same, 1.0 / width, 0.0).astype(BF16)
        mean = jnp.concatenate([mean, mean], axis=0)
        pieces = []
        for j in range(4):
            cols = slice(ROWS * j, ROWS * (j + 1))
            v = values[:, cols]
            m = jnp.dot(
                jnp.concatenate(split(v * v), axis=1), mean, preferred_element_type=F32
            )
            pieces.append((v * lax.rsqrt(m + 1e-06) * gain[:, cols]).astype(BF16))
        return jnp.concatenate(pieces, axis=1)

    conv_out = head_norm(bg_v[...] * conv, cgain_v[...], 64)
    loads[17].wait()
    for c in range(4):
        cpart_v[:, CH * c : CH * (c + 1)] = jnp.dot(
            conv_out, woc_v[:, CH * c : CH * (c + 1)], preferred_element_type=F32
        )

    sz[1]()
    az = [(pz[0] * jnp.exp(w), pz[1] * jnp.exp(w)) for w in expand([sz_v[k] for k in range(nz)])]
    loads[12].wait()
    start = (paired(init_v, (0,)), paired(init_v, (1,)))
    loads[14].wait()
    loads[18].wait()

    mz[1]()
    pre_z, _ = sweep(az, [take(mz_v, k) for k in range(nz)], start, z)
    entry = cadd(cmul(dx, cadd(cmul(dy, pre_z), pre_y)), pre_x)
    entry = cmul(enter, entry)
    sum_v[0], sum_v[1] = entry
    for r in range(PAIRS):
        span = slice(32 * r, 32 * r + 32)
        ce = cmul(
            (sum_v[0, r : r + 1, :], sum_v[1, r : r + 1, :]), (cw_v[span, 0:ROWS], cw_v[span, ROWS:])
        )
        at = 32 * (r % 4)
        for k, w in enumerate((ce[0], -ce[1])):
            lanes = slice(ROWS * k, ROWS * (k + 1))
            high, low = split(w)
            ce_v[r // 4, at : at + 32, lanes] = high
            ce_v[r // 4, ROWS + at : ROWS + at + 32, lanes] = low
    acts = []
    for j in range(4):
        cols = slice(ROWS * j, ROWS * (j + 1))
        span = slice(4 * ROWS * j, 4 * ROWS * (j + 1))
        pre = ypre_v[:, cols] + read_out(wposb_v[0, span, :], wposb_v[1, span, :], ce_v[j])
        acts.append(0.5 * pre * (1.0 + lax.erf(pre * math.sqrt(0.5))))
    sout_v[...] = head_norm(jnp.concatenate(acts, axis=1), sgain_v[...], 16)

    sends = []
    for c in range(4):
        cols = slice(CH * c, CH * (c + 1))
        part = jnp.dot(sout_v[...], wos_v[:, cols], preferred_element_type=F32) + cpart_v[:, cols]
        part_v[c] = part.astype(BF16)
        send = pltpu.make_async_remote_copy(
            part_v.at[c, pl.ds(other * 64, 64)],
            got_v.at[c],
            part_ss.at[c],
            part_rs.at[c],
            device_id={"tp": other},
        )
        send.start()
        sends.append(send)
    for c in range(4):
        cols = slice(CH * c, CH * (c + 1))
        sends[c].wait_recv()
        own = part_v[c, pl.ds(tp * 64, 64), :].astype(F32)
        out[:, cols] = (own + got_v[c].astype(F32)).astype(BF16)
    for c in range(4):
        sends[c].wait_send()
    tok_copy.wait_send()
    gain_copy.wait_send()
    pl.when(index + 1 < count)(tail_copy.wait_send)
    for ex in (sx, sy, sz, mx, my, mz):
        ex[2]()


def body(dims, *args):
    args = list(args)
    args[9] = jnp.swapaxes(args[9], 2, 3).reshape(2, CH, ENTRIES)
    args[10] = args[10].reshape(2, CH, ENTRIES)
    for k in (12, 13, 14):
        args[k] = args[k].reshape(1, CH)
    args = [pltpu.with_memory_space_constraint(a, pltpu.MemorySpace.HBM) for a in args]
    nz, ny, nx = dims
    anyspace = pl.BlockSpec(memory_space=pltpu.MemorySpace.HBM)
    vm = pltpu.VMEM
    dma = pltpu.SemaphoreType.DMA
    scratch = [
        vm((2, ROWS, HALF), BF16),
        vm((2, 1, HALF), BF16),
        vm((D, CH), BF16),
        vm((D, CH), BF16),
        vm((D, CH), BF16),
        vm((D, CH), BF16),
        vm((GROUPS, ENTRIES), F32),
        vm((GROUPS, ENTRIES), F32),
        vm((GROUPS, ROWS), F32),
        vm((2, CH, ENTRIES), F32),
        vm((2, CH, ENTRIES), F32),
        vm((2, GROUPS, ENTRIES), F32),
        vm((1, CH), F32),
        vm((1, CH), F32),
        vm((1, CH), F32),
        vm((3, CH), F32),
        vm((CH, D), BF16),
        vm((CH, D), BF16),
        vm((ROWS, CH), F32),
        vm((ROWS, CH), BF16),
        vm((4, 256, 256), BF16),
        vm((CH, 256), F32),
        vm((4, 256, 256), BF16),
        vm((2, PAIRS, ROWS, ROWS), F32),
        vm((4, 16, PAIRS, ROWS), F32),
        vm((4, ROWS, ROWS), F32),
        vm((2, PAIRS, ROWS, ROWS), F32),
        vm((2, PAIRS, ROWS, ROWS), F32),
        vm((2, PAIRS * ROWS, 256), BF16),
        vm((PAIRS, ROWS, 256), F32),
        vm((2, PAIRS, ROWS), F32),
        vm((256, ROWS), BF16),
        vm((ROWS, CH), F32),
        vm((ROWS + 8, CH), F32),
        vm((ROWS, CH), F32),
        vm((ROWS, D), F32),
        vm((ROWS, CH), BF16),
        vm((4, ROWS, CH), BF16),
        vm((4, 64, CH), BF16),
        vm((nx, 1, ROWS), F32),
        vm((ny, 1, ROWS), F32),
        vm((nz, 1, ROWS), F32),
        vm((nx, 32, ROWS), F32),
        vm((ny, 32, ROWS), F32),
        vm((nz, 32, ROWS), F32),
        dma((19,)),
        dma((4,)),
        dma((2,)),
        dma((4,)),
        dma((4,)),
        dma((2, nx)),
        dma((2, ny)),
        dma((2, nz)),
        dma((2, nx)),
        dma((2, ny)),
        dma((2, nz)),
        *[pltpu.SemaphoreType.REGULAR] * 5,
    ]
    return pl.pallas_call(
        functools.partial(kernel, dims),
        out_shape=jax.ShapeDtypeStruct((64, D), BF16),
        in_specs=[anyspace] * len(args),
        out_specs=pl.BlockSpec(memory_space=pltpu.MemorySpace.VMEM),
        scratch_shapes=scratch,
        compiler_params=pltpu.CompilerParams(
            collective_id=0, has_side_effects=True, vmem_limit_bytes=48 * 1024 * 1024
        ),
        name="layer",
    )(*args)


def solution(mesh):
    dims = SP_DIMS
    finer = Mesh(mesh.devices.reshape(*dims, mesh.shape["tp"]), (*SP, "tp"))
    placed = (
        P(SP, "tp"),
        P(None, "tp"),
        P(None, "tp"),
        P(None, "tp"),
        P(None, "tp"),
        P(None, "tp"),
        P("tp", None),
        P("tp", None),
        P("tp", SP),
        P(None, "tp", None, None),
        P(None, "tp", None, None),
        P(None, "tp", None),
        P("tp"),
        P("tp"),
        P("tp"),
        P(None, "tp"),
        P("tp", None),
        P("tp", None),
    )
    return jax.shard_map(
        functools.partial(body, dims),
        mesh=finer,
        in_specs=placed,
        out_specs=P((*SP, "tp"), None),
        check_vma=False,
    )
```

```python
import functools
import math

import jax
import jax.numpy as jnp
from jax import lax
from jax.experimental import pallas as pl
from jax.experimental.pallas import tpu as pltpu
from jax.sharding import Mesh
from jax.sharding import PartitionSpec as P

D = 2048
HALF = 1024
CH = 512
GROUPS = 32
ENTRIES = 64
ROWS = 128
PAIRS = 16
SP_DIMS = (8, 8, 4)
SP = ("sz", "sy", "sx")
F32 = jnp.float32
BF16 = jnp.bfloat16
HIGHEST = lax.Precision.HIGHEST


def cmul(a, b):
    return (a[0] * b[0] - a[1] * b[1], a[0] * b[1] + a[1] * b[0])


def cadd(a, b):
    return (a[0] + b[0], a[1] + b[1])


def expm1(v):
    series = 1.0 + v / 8.0
    for k in range(7, 1, -1):
        series = 1.0 + series * v / k
    return jnp.where(jnp.abs(v) < 0.3, v * series, jnp.exp(v) - 1.0)


def split(v):
    high = v.astype(BF16)
    return high, (v - high.astype(F32)).astype(BF16)


def iota(shape, dim):
    return lax.broadcasted_iota(jnp.int32, shape, dim)


def kernel(
    dims,
    tokens,
    in_gain,
    w_input,
    w_bgate,
    w_cgate,
    w_value,
    decay_rate,
    angle,
    decay_shift,
    b_input,
    c_output,
    initial,
    skip_gain,
    ssm_gain,
    conv_gain,
    conv_taps,
    w_out_ssm,
    w_out_conv,
    out,
    tok_v,
    gain_v,
    win_v,
    wb_v,
    wc_v,
    wv_v,
    rate_v,
    angle_v,
    shift_v,
    b_v,
    c_v,
    init_v,
    skip_v,
    sgain_v,
    cgain_v,
    taps_v,
    wos_v,
    woc_v,
    acc_v,
    u_v,
    bw_v,
    cw_v,
    ce_v,
    expf_v,
    at_v,
    bt_v,
    wneg_v,
    wpos_v,
    wposb_v,
    q_v,
    sum_v,
    mixed_v,
    ypre_v,
    pad_v,
    bg_v,
    cpart_v,
    sout_v,
    part_v,
    got_v,
    sx_v,
    sy_v,
    sz_v,
    mx_v,
    my_v,
    mz_v,
    load_sem,
    tok_sem,
    tail_sem,
    part_ss,
    part_rs,
    sx_sem,
    sy_sem,
    sz_sem,
    mx_sem,
    my_sem,
    mz_sem,
    ring2,
    ring3,
    zring2,
    zring3,
    zring4,
):
    nz, ny, nx = dims
    z, y, x = (lax.axis_index(a) for a in SP)
    tp = lax.axis_index("tp")
    other = 1 - tp
    coords = {"sz": (z, nz), "sy": (y, ny), "sx": (x, nx)}

    pairs = [
        (tokens, tok_v.at[tp]),
        (in_gain, gain_v.at[tp]),
        (w_input.at[pl.ds(tp * HALF, HALF)], win_v.at[pl.ds(tp * HALF, HALF)]),
        (decay_shift, shift_v),
        (decay_rate, rate_v),
        (angle, angle_v),
        (w_input.at[pl.ds(other * HALF, HALF)], win_v.at[pl.ds(other * HALF, HALF)]),
        (b_input, b_v),
        (w_cgate, wc_v),
        (w_value, wv_v),
        (c_output, c_v),
        (w_bgate, wb_v),
        (initial, init_v),
        (skip_gain, skip_v),
        (ssm_gain, sgain_v),
        (conv_gain, cgain_v),
        (conv_taps, taps_v),
        (w_out_conv, woc_v),
        (w_out_ssm, wos_v),
    ]
    loads = [pltpu.make_async_copy(s, d, load_sem.at[k]) for k, (s, d) in enumerate(pairs)]
    for k in (0, 1, 3, 4, 5, 2, 7, 6):
        loads[k].start()

    def near(axis):
        n = coords[axis][1]
        return [] if n == 1 else ([1] if n == 2 else [1, n - 1])

    def at_step(axis, step):
        here, n = coords[axis]
        return {axis: lax.rem(here + step, n)}

    around = [at_step(a, s) for a in ("sy", "sx") for s in near(a)]
    far = [at_step("sx", s) for s in near("sx")]
    far += [at_step("sy", s) for s in (2, 6) if ny == 8]

    def tell(sem, step, above=True):
        @pl.when(z >= step)
        def _():
            pl.semaphore_signal(sem, inc=1, device_id={"sz": z - step})

        if above:

            @pl.when(z + step < nz)
            def _():
                pl.semaphore_signal(sem, inc=1, device_id={"sz": z + step})

    def beside(step):
        return jnp.where(z + step < nz, 1, 0) + jnp.where(z >= step, 1, 0)

    barrier = pltpu.get_barrier_semaphore()
    for dev in [{"tp": other}] + around:
        pl.semaphore_signal(barrier, inc=1, device_id=dev)
    tell(barrier, 1)

    loads[0].wait()
    loads[1].wait()
    pl.semaphore_wait(barrier, 1 + len(around) + beside(1))

    tok_copy = pltpu.make_async_remote_copy(
        tok_v.at[tp], tok_v.at[tp], tok_sem.at[0], tok_sem.at[1], device_id={"tp": other}
    )
    gain_copy = pltpu.make_async_remote_copy(
        gain_v.at[tp], gain_v.at[tp], tok_sem.at[2], tok_sem.at[3], device_id={"tp": other}
    )
    tok_copy.start()
    gain_copy.start()
    for dev in around:
        pl.semaphore_signal(ring2, inc=1, device_id=dev)
    if nz > 2:
        tell(zring2, 1)
    for k in range(8, len(loads)):
        loads[k].start()

    def exchange(buf, sems, axis, later):
        here, n = coords[axis]
        order = sorted(range(1, n), key=lambda s: -min(s, n - s))

        def copy(step):
            return pltpu.make_async_remote_copy(
                buf.at[here],
                buf.at[here],
                sems.at[0, step],
                sems.at[1, step],
                device_id=at_step(axis, step),
            )

        def start(first=1, end=n):
            for s in order:
                if not first <= s < end:
                    continue
                if later:
                    pl.when(here + s < n)(copy(s).start)
                else:
                    copy(s).start()

        def incoming(step):
            slot = lax.rem(here + n - step, n)
            return pltpu.make_async_remote_copy(
                buf.at[slot],
                buf.at[slot],
                sems.at[0, step],
                sems.at[1, step],
                device_id=at_step(axis, step),
            )

        def wait_recv():
            for s in range(1, n):
                if later:
                    pl.when(here >= s)(incoming(s).wait_recv)
                else:
                    incoming(s).wait_recv()

        def wait_send():
            for s in range(1, n):
                if later:
                    pl.when(here + s < n)(copy(s).wait_send)
                else:
                    copy(s).wait_send()

        return start, wait_recv, wait_send

    sx = exchange(sx_v, sx_sem, "sx", False)
    sy = exchange(sy_v, sy_sem, "sy", False)
    sz = exchange(sz_v, sz_sem, "sz", True)
    mx = exchange(mx_v, mx_sem, "sx", False)
    my = exchange(my_v, my_sem, "sy", False)
    mz = exchange(mz_v, mz_sem, "sz", True)

    def half(which):
        floats = tok_v[which].astype(F32)
        scaled = (floats * gain_v[which].astype(F32)).astype(BF16)
        return scaled, jnp.sum(floats * floats, axis=1, keepdims=True)

    loads[3].wait()
    tri = (iota((ROWS, ROWS), 0) >= iota((ROWS, ROWS), 1)).astype(F32)
    shifts = jnp.concatenate([shift_v[...], jnp.zeros((ROWS - GROUPS, ROWS), F32)], axis=0)
    logs = lax.dot_general(
        tri, shifts, (((1,), (1,)), ((), ())), precision=HIGHEST, preferred_element_type=F32
    )
    sigma = logs[ROWS - 1 : ROWS]
    mid = logs[ROWS // 2 - 1 : ROWS // 2]
    sx_v[x] = sigma

    loads[4].wait()
    loads[5].wait()

    def paired(ref, lead=()):
        even = ref[(*lead, pl.ds(0, PAIRS, 2), slice(None))]
        odd = ref[(*lead, pl.ds(1, PAIRS, 2), slice(None))]
        return jnp.concatenate([even, odd], axis=1)

    rate = paired(rate_v)
    theta = paired(angle_v)

    def power(k):
        mag = jnp.exp(-rate * float(k))
        ph = theta * float(k)
        return (mag * jnp.cos(ph), mag * jnp.sin(ph))

    cos1, sin1 = jnp.cos(theta), jnp.sin(theta)
    unit = (cos1, sin1)
    lane = iota((1, ROWS), 1)
    grp = iota((PAIRS, ROWS), 0)
    grp_lane = iota((PAIRS, ROWS), 1)
    spread_h = (
        (iota((ROWS, ROWS), 0) % 2 == iota((ROWS, ROWS), 1) // ENTRIES)
        & (iota((ROWS, ROWS), 0) < GROUPS)
    ).astype(F32)

    def expand(rows):
        blocks = [jnp.where(grp_lane // 2 == grp, row, 0.0) for row in rows]
        wide = jnp.dot(
            jnp.concatenate(blocks, axis=0), spread_h, precision=HIGHEST, preferred_element_type=F32
        )
        return [wide[PAIRS * k : PAIRS * (k + 1)] for k in range(len(rows))]

    keep = lane < GROUPS
    ratio = jnp.concatenate([jnp.exp(mid - logs), jnp.exp(logs - mid)], axis=0)
    ratio = jnp.where(keep, ratio, 0.0)
    hi = ratio.astype(BF16)
    lo = ratio - hi.astype(F32)
    both = hi.astype(F32) + pltpu.roll(lo, GROUPS, 1)
    both = both.astype(BF16)
    mixed_v[...] = both

    def spread(part):
        for k in range(PAIRS // 2):
            src = iota((ROWS, 256), 0)
            dst = iota((ROWS, 256), 1) + 256 * k
            pick = ((src % GROUPS == dst // ENTRIES) & (src < 2 * GROUPS)).astype(F32).astype(BF16)
            wide = jnp.dot(
                mixed_v[ROWS * part : ROWS * (part + 1), :], pick, preferred_element_type=F32
            )
            expf_v[part, 2 * k] = wide[:, :ROWS]
            expf_v[part, 2 * k + 1] = wide[:, ROWS:]

    spread(0)

    ph = unit
    for b in range(8):
        bt_v[0, pl.ds(b, PAIRS, 8), :] = ph[0]
        bt_v[1, pl.ds(b, PAIRS, 8), :] = ph[1]
        mag = jnp.exp(-rate * float(b + 1))
        bt_v[2, pl.ds(b, PAIRS, 8), :] = mag
        bt_v[3, pl.ds(b, PAIRS, 8), :] = 1.0 / mag
        ph8 = ph
        ph = cmul(ph, unit)
    ph = (jnp.ones_like(cos1), jnp.zeros_like(cos1))
    for a in range(8, 16):
        at_v[0, a], at_v[1, a] = ph
        mag = jnp.exp(-rate * float(8 * (a - 8)))
        at_v[2, a], at_v[3, a] = mag, 1.0 / mag
        ph = cmul(ph, ph8)
        back = 16 - (a + 1)
        at_v[0, back], at_v[1, back] = ph[0], -ph[1]
        mag = jnp.exp(rate * float(8 * (8 - back)))
        at_v[2, back], at_v[3, back] = mag, 1.0 / mag

    def table(part, store):
        @pl.loop(0, PAIRS)
        def _(r):
            cb, sb, mb = (bt_v[k, pl.ds(r * 8, 8), :] for k in (0, 1, 3 - part))
            for a in range(16):
                ca, sa, ma = (
                    jnp.broadcast_to(at_v[k, a, pl.ds(r, 1), :], (8, ROWS)) for k in (0, 1, 3 - part)
                )
                c, s = cmul((ca, sa), (cb, sb))
                span = slice(8 * a, 8 * a + 8)
                store(r, span, c, s, ma * mb * expf_v[part, r, span, :])

    def backward(r, span, c, s, scale):
        wneg_v[0, r, span, :] = c * scale
        wneg_v[1, r, span, :] = -s * scale

    def forward(r, span, c, s, scale):
        wpos_v[0, r, span, :] = c * scale
        wpos_v[1, r, span, :] = s * scale

    table(0, backward)
    mid_wide, rest_wide = expand([mid, sigma - mid])
    p64 = power(64)
    end = cmul((at_v[0, 15], at_v[1, 15]), ph8)
    fall = jnp.exp(rest_wide) * jnp.exp(-rate * 64.0)
    last = (end[0] * fall, end[1] * fall)
    enter = (p64[0] * jnp.exp(mid_wide), p64[1] * jnp.exp(mid_wide))

    loads[7].wait()
    dec = expm1(-rate) * cos1 - 2.0 * jnp.sin(0.5 * theta) ** 2
    ims = jnp.exp(-rate) * sin1
    den = rate * rate + theta * theta
    zr = (ims * theta - dec * rate) / den
    zi = -(ims * rate + dec * theta) / den
    sum_v[0], sum_v[1] = zr, zi
    mask = iota((32, ROWS), 0) // 16 == iota((32, ROWS), 1) // ENTRIES
    for r in range(PAIRS):
        span = slice(32 * r, 32 * r + 32)
        br, bi = b_v[0, span, :], b_v[1, span, :]
        br = jnp.concatenate([br, br], axis=1)
        bi = jnp.concatenate([bi, bi], axis=1)
        wr, wi = cmul((sum_v[0, r : r + 1, :], sum_v[1, r : r + 1, :]), (br, bi))
        at = 32 * (r % 4)
        for k, w in enumerate((wr, wi)):
            lanes = slice(ROWS * k, ROWS * (k + 1))
            high, low = split(jnp.where(mask, w, 0.0))
            bw_v[r // 4, at : at + 32, lanes] = high
            bw_v[r // 4, ROWS + at : ROWS + at + 32, lanes] = low

    own_scaled, own_sq = half(tp)
    loads[2].wait()
    acc_v[...] = jnp.dot(
        own_scaled, win_v[pl.ds(tp * HALF, HALF), :], preferred_element_type=F32
    )

    if around:
        pl.semaphore_wait(ring2, len(around))
    sx[0]()
    for dev in far:
        pl.semaphore_signal(ring3, inc=1, device_id=dev)
    if nz > 2:
        pl.semaphore_wait(zring2, beside(1))
        tell(zring3, 2)

    tok_copy.wait_recv()
    gain_copy.wait_recv()
    far_scaled, far_sq = half(other)
    inv = lax.rsqrt((own_sq + far_sq) / D + 1e-06)
    loads[6].wait()
    acc = acc_v[...] + jnp.dot(
        far_scaled, win_v[pl.ds(other * HALF, HALF), :], preferred_element_type=F32
    )
    u_v[...] = (acc * inv).astype(BF16)

    quarter = iota((ROWS, ROWS), 1) // 32
    for j in range(4):
        uj = u_v[:, ROWS * j : ROWS * (j + 1)]
        stacked = jnp.concatenate(
            [jnp.where(quarter == i, uj, jnp.zeros_like(uj)) for i in range(4)], axis=0
        )
        drive = jnp.dot(
            jnp.concatenate([stacked, stacked], axis=1), bw_v[j], preferred_element_type=F32
        )
        for i in range(4):
            r = 4 * j + i
            d = drive[ROWS * i : ROWS * (i + 1)]
            q = cmul((wneg_v[0, r], wneg_v[1, r]), (d[:, :ROWS], d[:, ROWS:]))
            sum_v[0, r : r + 1, :] = jnp.sum(q[0], axis=0, keepdims=True)
            sum_v[1, r : r + 1, :] = jnp.sum(q[1], axis=0, keepdims=True)
            q_v[r, :, 0:ROWS] = q[0]
            q_v[r, :, ROWS:] = q[1]
    mine = cmul(last, (sum_v[0], sum_v[1]))

    def put(buf, index, value):
        buf[index, 0:PAIRS, :] = value[0]
        buf[index, PAIRS : 2 * PAIRS, :] = value[1]

    def take(buf, index):
        return (buf[index, 0:PAIRS, :], buf[index, PAIRS : 2 * PAIRS, :])

    put(mx_v, x, mine)
    mx[0]()

    spread(1)
    table(1, forward)
    def project(w):
        acc = jnp.dot(own_scaled, w[pl.ds(tp * HALF, HALF), :], preferred_element_type=F32)
        acc = acc + jnp.dot(far_scaled, w[pl.ds(other * HALF, HALF), :], preferred_element_type=F32)
        return (acc * inv).astype(BF16).astype(F32)

    loads[8].wait()
    loads[9].wait()
    pad_v[8:, :] = project(wc_v) * project(wv_v)
    sx[1]()
    rows = [sx_v[k] for k in range(nx)]
    rho = functools.reduce(jnp.add, rows)
    sy_v[y] = rho
    if far:
        pl.semaphore_wait(ring3, len(far))
    sy[0]()
    if nz > 2:

        @pl.when(beside(2) > 0)
        def _():
            pl.semaphore_wait(zring3, beside(2))

    if nz > 4:
        tell(zring4, 4, above=False)

    index = (z * ny + y) * nx + x
    count = nz * ny * nx
    x1 = lax.rem(x + 1, nx)
    carry = x + 1 == nx
    y1 = jnp.where(carry, lax.rem(y + 1, ny), y)
    z1 = jnp.where(carry & (y + 1 == ny), lax.rem(z + 1, nz), z)
    tail_copy = pltpu.make_async_remote_copy(
        pad_v.at[ROWS : ROWS + 8],
        pad_v.at[0:8],
        tail_sem.at[0],
        tail_sem.at[1],
        device_id={"sz": z1, "sy": y1, "sx": x1},
    )
    pl.when(index + 1 < count)(tail_copy.start)

    wide = expand(rows)
    p128 = power(ROWS)
    ax = [(p128[0] * jnp.exp(w), p128[1] * jnp.exp(w)) for w in wide]

    def sweep(steps, values, start, here):
        total = before = start
        for k in range(len(steps)):
            if k:
                before = tuple(jnp.where(here == k, t, b) for t, b in zip(total, before))
            total = cmul(steps[k], total)
            if values is not None:
                total = cadd(total, values[k])
        return before, total

    one = (jnp.ones_like(cos1), jnp.zeros_like(cos1))
    zero = (jnp.zeros_like(cos1), jnp.zeros_like(cos1))
    dx, _ = sweep(ax, None, one, x)

    mx[1]()
    pre_x, row_total = sweep(ax, [take(mx_v, k) for k in range(nx)], zero, x)
    put(my_v, y, row_total)
    my[0]()

    loads[10].wait()
    for r in range(PAIRS):
        span = slice(32 * r, 32 * r + 32)
        cr, ci = c_v[0, span, :], c_v[1, span, :]
        cw_v[span, 0:ROWS] = jnp.where(mask, jnp.concatenate([cr, cr], axis=1), 0.0)
        cw_v[span, ROWS:] = jnp.where(mask, jnp.concatenate([ci, ci], axis=1), 0.0)
    tri16 = jnp.concatenate([tri.astype(BF16), tri.astype(BF16)], axis=1)
    sign = jnp.where(iota((1, 256), 1) < ROWS, 1.0, -1.0)
    nt = (((1,), (1,)), ((), ()))

    def gathered(wide):
        total = jnp.where(quarter == 0, wide[0:ROWS], 0.0)
        for i in range(1, 4):
            total = jnp.where(quarter == i, wide[ROWS * i : ROWS * (i + 1)], total)
        return total

    def read_out(high, low, weights):
        wide = lax.dot_general(high, weights, nt, preferred_element_type=F32)
        rest = lax.dot_general(low, weights[0:ROWS], nt, preferred_element_type=F32)
        return gathered(wide[:, :ROWS] + wide[:, ROWS:] + rest)

    loads[13].wait()
    for j in range(4):
        highs, lows = [], []
        for i in range(4):
            r = 4 * j + i
            pre = jnp.dot(
                tri16, jnp.concatenate(split(q_v[r]), axis=0), preferred_element_type=F32
            )
            st = cmul((wpos_v[0, r], wpos_v[1, r]), (pre[:, :ROWS], pre[:, ROWS:]))
            high, low = zip(*(split(part) for part in st))
            highs.append(jnp.concatenate(high, axis=1))
            lows.append(jnp.concatenate(low, axis=1))
            for k in range(2):
                lanes = slice(ROWS * k, ROWS * (k + 1))
                span = slice(ROWS * r, ROWS * (r + 1))
                wposb_v[0, span, lanes], wposb_v[1, span, lanes] = split(wpos_v[k, r])
        cols = slice(ROWS * j, ROWS * (j + 1))
        weights = jnp.concatenate(split(cw_v[cols, :] * sign), axis=0)
        read = read_out(jnp.concatenate(highs, axis=0), jnp.concatenate(lows, axis=0), weights)
        ypre_v[:, cols] = read + skip_v[:, cols] * u_v[:, cols].astype(F32)

    loads[11].wait()
    bg_v[...] = project(wb_v)

    @pl.when(index == 0)
    def _():
        pad_v[0:8, :] = jnp.zeros((8, CH), F32)

    pl.when(index > 0)(tail_copy.wait_recv)
    loads[15].wait()
    loads[16].wait()
    conv = pad_v[6 : 6 + ROWS, :] * taps_v[0:1, :]
    conv = conv + pad_v[7 : 7 + ROWS, :] * taps_v[1:2, :]
    conv = conv + pad_v[8 : 8 + ROWS, :] * taps_v[2:3, :]

    def head_norm(values, gain, width):
        same = iota((ROWS, ROWS), 0) // width == iota((ROWS, ROWS), 1) // width
        mean = jnp.where(same, 1.0 / width, 0.0).astype(BF16)
        mean = jnp.concatenate([mean, mean], axis=0)
        pieces = []
        for j in range(4):
            cols = slice(ROWS * j, ROWS * (j + 1))
            v = values[:, cols]
            m = jnp.dot(
                jnp.concatenate(split(v * v), axis=1), mean, preferred_element_type=F32
            )
            pieces.append((v * lax.rsqrt(m + 1e-06) * gain[:, cols]).astype(BF16))
        return jnp.concatenate(pieces, axis=1)

    conv_out = head_norm(bg_v[...] * conv, cgain_v[...], 64)
    loads[17].wait()
    for c in range(4):
        cpart_v[:, CH * c : CH * (c + 1)] = jnp.dot(
            conv_out, woc_v[:, CH * c : CH * (c + 1)], preferred_element_type=F32
        )

    sy[1]()
    rows = [sy_v[k] for k in range(ny)]
    pi = functools.reduce(jnp.add, rows)
    sz_v[z] = pi
    sz[0](1, 5)
    p512 = power(ROWS * nx)
    ay = [(p512[0] * jnp.exp(w), p512[1] * jnp.exp(w)) for w in expand(rows)]
    dy, _ = sweep(ay, None, one, y)
    pz = power(ROWS * nx * ny)

    my[1]()
    pre_y, plane_total = sweep(ay, [take(my_v, k) for k in range(ny)], zero, y)
    put(mz_v, z, plane_total)
    mz[0](1, 5)
    if nz > 4:

        @pl.when(z + 4 < nz)
        def _():
            pl.semaphore_wait(zring4, 1)

        sz[0](5, nz)
        mz[0](5, nz)

    sz[1]()
    az = [(pz[0] * jnp.exp(w), pz[1] * jnp.exp(w)) for w in expand([sz_v[k] for k in range(nz)])]
    loads[12].wait()
    start = (paired(init_v, (0,)), paired(init_v, (1,)))
    loads[14].wait()
    loads[18].wait()

    tok_copy.wait_send()
    gain_copy.wait_send()
    pl.when(index + 1 < count)(tail_copy.wait_send)
    for ex in (sx, mx, sy, my):
        ex[2]()

    mz[1]()
    pre_z, _ = sweep(az, [take(mz_v, k) for k in range(nz)], start, z)
    entry = cadd(cmul(dx, cadd(cmul(dy, pre_z), pre_y)), pre_x)
    entry = cmul(enter, entry)
    sum_v[0], sum_v[1] = entry
    for r in range(PAIRS):
        span = slice(32 * r, 32 * r + 32)
        ce = cmul(
            (sum_v[0, r : r + 1, :], sum_v[1, r : r + 1, :]), (cw_v[span, 0:ROWS], cw_v[span, ROWS:])
        )
        at = 32 * (r % 4)
        for k, w in enumerate((ce[0], -ce[1])):
            lanes = slice(ROWS * k, ROWS * (k + 1))
            high, low = split(w)
            ce_v[r // 4, at : at + 32, lanes] = high
            ce_v[r // 4, ROWS + at : ROWS + at + 32, lanes] = low
    acts = []
    for j in range(4):
        cols = slice(ROWS * j, ROWS * (j + 1))
        span = slice(4 * ROWS * j, 4 * ROWS * (j + 1))
        pre = ypre_v[:, cols] + read_out(wposb_v[0, span, :], wposb_v[1, span, :], ce_v[j])
        acts.append(0.5 * pre * (1.0 + lax.erf(pre * math.sqrt(0.5))))
    sout_v[...] = head_norm(jnp.concatenate(acts, axis=1), sgain_v[...], 16)

    sends = []
    for c in range(4):
        cols = slice(CH * c, CH * (c + 1))
        part = jnp.dot(sout_v[...], wos_v[:, cols], preferred_element_type=F32) + cpart_v[:, cols]
        part_v[c] = part.astype(BF16)
        send = pltpu.make_async_remote_copy(
            part_v.at[c, pl.ds(other * 64, 64)],
            got_v.at[c],
            part_ss.at[c],
            part_rs.at[c],
            device_id={"tp": other},
        )
        send.start()
        sends.append(send)
    sz[2]()
    mz[2]()
    for c in range(4):
        cols = slice(CH * c, CH * (c + 1))
        sends[c].wait_recv()
        own = part_v[c, pl.ds(tp * 64, 64), :].astype(F32)
        out[:, cols] = (own + got_v[c].astype(F32)).astype(BF16)
    for c in range(4):
        sends[c].wait_send()


def body(dims, *args):
    args = list(args)
    args[9] = jnp.swapaxes(args[9], 2, 3).reshape(2, CH, ENTRIES)
    args[10] = args[10].reshape(2, CH, ENTRIES)
    for k in (12, 13, 14):
        args[k] = args[k].reshape(1, CH)
    args = [pltpu.with_memory_space_constraint(a, pltpu.MemorySpace.HBM) for a in args]
    nz, ny, nx = dims
    anyspace = pl.BlockSpec(memory_space=pltpu.MemorySpace.HBM)
    vm = pltpu.VMEM
    dma = pltpu.SemaphoreType.DMA
    scratch = [
        vm((2, ROWS, HALF), BF16),
        vm((2, 1, HALF), BF16),
        vm((D, CH), BF16),
        vm((D, CH), BF16),
        vm((D, CH), BF16),
        vm((D, CH), BF16),
        vm((GROUPS, ENTRIES), F32),
        vm((GROUPS, ENTRIES), F32),
        vm((GROUPS, ROWS), F32),
        vm((2, CH, ENTRIES), F32),
        vm((2, CH, ENTRIES), F32),
        vm((2, GROUPS, ENTRIES), F32),
        vm((1, CH), F32),
        vm((1, CH), F32),
        vm((1, CH), F32),
        vm((3, CH), F32),
        vm((CH, D), BF16),
        vm((CH, D), BF16),
        vm((ROWS, CH), F32),
        vm((ROWS, CH), BF16),
        vm((4, 256, 256), BF16),
        vm((CH, 256), F32),
        vm((4, 256, 256), BF16),
        vm((2, PAIRS, ROWS, ROWS), F32),
        vm((4, 16, PAIRS, ROWS), F32),
        vm((4, ROWS, ROWS), F32),
        vm((2, PAIRS, ROWS, ROWS), F32),
        vm((2, PAIRS, ROWS, ROWS), F32),
        vm((2, PAIRS * ROWS, 256), BF16),
        vm((PAIRS, ROWS, 256), F32),
        vm((2, PAIRS, ROWS), F32),
        vm((256, ROWS), BF16),
        vm((ROWS, CH), F32),
        vm((ROWS + 8, CH), F32),
        vm((ROWS, CH), F32),
        vm((ROWS, D), F32),
        vm((ROWS, CH), BF16),
        vm((4, ROWS, CH), BF16),
        vm((4, 64, CH), BF16),
        vm((nx, 1, ROWS), F32),
        vm((ny, 1, ROWS), F32),
        vm((nz, 1, ROWS), F32),
        vm((nx, 32, ROWS), F32),
        vm((ny, 32, ROWS), F32),
        vm((nz, 32, ROWS), F32),
        dma((19,)),
        dma((4,)),
        dma((2,)),
        dma((4,)),
        dma((4,)),
        dma((2, nx)),
        dma((2, ny)),
        dma((2, nz)),
        dma((2, nx)),
        dma((2, ny)),
        dma((2, nz)),
        *[pltpu.SemaphoreType.REGULAR] * 5,
    ]
    return pl.pallas_call(
        functools.partial(kernel, dims),
        out_shape=jax.ShapeDtypeStruct((64, D), BF16),
        in_specs=[anyspace] * len(args),
        out_specs=pl.BlockSpec(memory_space=pltpu.MemorySpace.VMEM),
        scratch_shapes=scratch,
        compiler_params=pltpu.CompilerParams(
            collective_id=0, has_side_effects=True, vmem_limit_bytes=48 * 1024 * 1024
        ),
        name="layer",
    )(*args)


def solution(mesh):
    dims = SP_DIMS
    finer = Mesh(mesh.devices.reshape(*dims, mesh.shape["tp"]), (*SP, "tp"))
    placed = (
        P(SP, "tp"),
        P(None, "tp"),
        P(None, "tp"),
        P(None, "tp"),
        P(None, "tp"),
        P(None, "tp"),
        P("tp", None),
        P("tp", None),
        P("tp", SP),
        P(None, "tp", None, None),
        P(None, "tp", None, None),
        P(None, "tp", None),
        P("tp"),
        P("tp"),
        P("tp"),
        P(None, "tp"),
        P("tp", None),
        P("tp", None),
    )
    return jax.shard_map(
        functools.partial(body, dims),
        mesh=finer,
        in_specs=placed,
        out_specs=P((*SP, "tp"), None),
        check_vma=False,
    )
```

```python
import functools
import math

import jax
import jax.numpy as jnp
from jax import lax
from jax.experimental import pallas as pl
from jax.experimental.pallas import tpu as pltpu
from jax.sharding import Mesh
from jax.sharding import PartitionSpec as P

D = 2048
HALF = 1024
CH = 512
GROUPS = 32
ENTRIES = 64
ROWS = 128
PAIRS = 16
SP_DIMS = (8, 8, 4)
SP = ("sz", "sy", "sx")
F32 = jnp.float32
BF16 = jnp.bfloat16
HIGHEST = lax.Precision.HIGHEST


def cmul(a, b):
    return (a[0] * b[0] - a[1] * b[1], a[0] * b[1] + a[1] * b[0])


def cadd(a, b):
    return (a[0] + b[0], a[1] + b[1])


def expm1(v):
    series = 1.0 + v / 8.0
    for k in range(7, 1, -1):
        series = 1.0 + series * v / k
    return jnp.where(jnp.abs(v) < 0.3, v * series, jnp.exp(v) - 1.0)


def split(v):
    high = v.astype(BF16)
    return high, (v - high.astype(F32)).astype(BF16)


def iota(shape, dim):
    return lax.broadcasted_iota(jnp.int32, shape, dim)


def kernel(
    dims,
    tokens,
    in_gain,
    w_input,
    w_bgate,
    w_cgate,
    w_value,
    decay_rate,
    angle,
    decay_shift,
    b_input,
    c_output,
    initial,
    skip_gain,
    ssm_gain,
    conv_gain,
    conv_taps,
    w_out_ssm,
    w_out_conv,
    out,
    tok_v,
    gain_v,
    win_v,
    wb_v,
    wc_v,
    wv_v,
    rate_v,
    angle_v,
    shift_v,
    b_v,
    c_v,
    init_v,
    skip_v,
    sgain_v,
    cgain_v,
    taps_v,
    wos_v,
    woc_v,
    acc_v,
    u_v,
    bw_v,
    cw_v,
    ce_v,
    expf_v,
    at_v,
    bt_v,
    wneg_v,
    wpos_v,
    wposb_v,
    q_v,
    sum_v,
    mixed_v,
    ypre_v,
    pad_v,
    bg_v,
    cpart_v,
    sout_v,
    part_v,
    got_v,
    sx_v,
    sy_v,
    sz_v,
    mx_v,
    my_v,
    mz_v,
    load_sem,
    tok_sem,
    tail_sem,
    part_ss,
    part_rs,
    sx_sem,
    sy_sem,
    sz_sem,
    mx_sem,
    my_sem,
    mz_sem,
    ring2,
    ring3,
    zring2,
    zring3,
    zring4,
):
    nz, ny, nx = dims
    z, y, x = (lax.axis_index(a) for a in SP)
    tp = lax.axis_index("tp")
    other = 1 - tp
    coords = {"sz": (z, nz), "sy": (y, ny), "sx": (x, nx)}

    pairs = [
        (tokens, tok_v.at[tp]),
        (in_gain, gain_v.at[tp]),
        (w_input.at[pl.ds(tp * HALF, HALF)], win_v.at[pl.ds(tp * HALF, HALF)]),
        (decay_shift, shift_v),
        (decay_rate, rate_v),
        (angle, angle_v),
        (w_input.at[pl.ds(other * HALF, HALF)], win_v.at[pl.ds(other * HALF, HALF)]),
        (b_input, b_v),
        (w_cgate, wc_v),
        (w_value, wv_v),
        (c_output, c_v),
        (w_bgate, wb_v),
        (initial, init_v),
        (skip_gain, skip_v),
        (ssm_gain, sgain_v),
        (conv_gain, cgain_v),
        (conv_taps, taps_v),
        (w_out_conv, woc_v),
        (w_out_ssm, wos_v),
    ]
    loads = [pltpu.make_async_copy(s, d, load_sem.at[k]) for k, (s, d) in enumerate(pairs)]
    for k in (0, 1, 3, 4, 5, 2, 7, 6):
        loads[k].start()

    def near(axis):
        n = coords[axis][1]
        return [] if n == 1 else ([1] if n == 2 else [1, n - 1])

    def at_step(axis, step):
        here, n = coords[axis]
        return {axis: lax.rem(here + step, n)}

    around = [at_step(a, s) for a in ("sy", "sx") for s in near(a)]
    far = [at_step("sx", s) for s in near("sx")]
    far += [at_step("sy", s) for s in (2, 6) if ny == 8]

    def tell(sem, step):
        @pl.when(z >= step)
        def _():
            pl.semaphore_signal(sem, inc=1, device_id={"sz": z - step})

        @pl.when(z + step < nz)
        def _():
            pl.semaphore_signal(sem, inc=1, device_id={"sz": z + step})

    def beside(step):
        return jnp.where(z + step < nz, 1, 0) + jnp.where(z >= step, 1, 0)

    barrier = pltpu.get_barrier_semaphore()
    for dev in [{"tp": other}] + around:
        pl.semaphore_signal(barrier, inc=1, device_id=dev)
    tell(barrier, 1)

    loads[0].wait()
    loads[1].wait()
    pl.semaphore_wait(barrier, 1 + len(around) + beside(1))

    tok_copy = pltpu.make_async_remote_copy(
        tok_v.at[tp], tok_v.at[tp], tok_sem.at[0], tok_sem.at[1], device_id={"tp": other}
    )
    gain_copy = pltpu.make_async_remote_copy(
        gain_v.at[tp], gain_v.at[tp], tok_sem.at[2], tok_sem.at[3], device_id={"tp": other}
    )
    tok_copy.start()
    gain_copy.start()
    for dev in around:
        pl.semaphore_signal(ring2, inc=1, device_id=dev)
    if nz > 2:
        tell(zring2, 1)
    for k in range(8, len(loads)):
        loads[k].start()

    def exchange(buf, sems, axis, later):
        here, n = coords[axis]
        order = sorted(range(1, n), key=lambda s: -min(s, n - s))

        def copy(step):
            return pltpu.make_async_remote_copy(
                buf.at[here],
                buf.at[here],
                sems.at[0, step],
                sems.at[1, step],
                device_id=at_step(axis, step),
            )

        def start(first=1, end=n):
            for s in order:
                if not first <= s < end:
                    continue
                if later:
                    pl.when(here + s < n)(copy(s).start)
                else:
                    copy(s).start()

        def incoming(step):
            slot = lax.rem(here + n - step, n)
            return pltpu.make_async_remote_copy(
                buf.at[slot],
                buf.at[slot],
                sems.at[0, step],
                sems.at[1, step],
                device_id=at_step(axis, step),
            )

        def wait_recv():
            for s in range(1, n):
                if later:
                    pl.when(here >= s)(incoming(s).wait_recv)
                else:
                    incoming(s).wait_recv()

        def wait_send():
            for s in range(1, n):
                if later:
                    pl.when(here + s < n)(copy(s).wait_send)
                else:
                    copy(s).wait_send()

        return start, wait_recv, wait_send

    sx = exchange(sx_v, sx_sem, "sx", False)
    sy = exchange(sy_v, sy_sem, "sy", False)
    sz = exchange(sz_v, sz_sem, "sz", True)
    mx = exchange(mx_v, mx_sem, "sx", False)
    my = exchange(my_v, my_sem, "sy", False)
    mz = exchange(mz_v, mz_sem, "sz", True)

    def half(which):
        floats = tok_v[which].astype(F32)
        scaled = (floats * gain_v[which].astype(F32)).astype(BF16)
        return scaled, jnp.sum(floats * floats, axis=1, keepdims=True)

    loads[3].wait()
    tri = (iota((ROWS, ROWS), 0) >= iota((ROWS, ROWS), 1)).astype(F32)
    shifts = jnp.concatenate([shift_v[...], jnp.zeros((ROWS - GROUPS, ROWS), F32)], axis=0)
    logs = lax.dot_general(
        tri, shifts, (((1,), (1,)), ((), ())), precision=HIGHEST, preferred_element_type=F32
    )
    sigma = logs[ROWS - 1 : ROWS]
    mid = logs[ROWS // 2 - 1 : ROWS // 2]
    sx_v[x] = sigma

    loads[4].wait()
    loads[5].wait()

    def paired(ref, lead=()):
        even = ref[(*lead, pl.ds(0, PAIRS, 2), slice(None))]
        odd = ref[(*lead, pl.ds(1, PAIRS, 2), slice(None))]
        return jnp.concatenate([even, odd], axis=1)

    rate = paired(rate_v)
    theta = paired(angle_v)

    def power(k):
        mag = jnp.exp(-rate * float(k))
        ph = theta * float(k)
        return (mag * jnp.cos(ph), mag * jnp.sin(ph))

    cos1, sin1 = jnp.cos(theta), jnp.sin(theta)
    unit = (cos1, sin1)
    lane = iota((1, ROWS), 1)
    grp = iota((PAIRS, ROWS), 0)
    grp_lane = iota((PAIRS, ROWS), 1)
    spread_h = (
        (iota((ROWS, ROWS), 0) % 2 == iota((ROWS, ROWS), 1) // ENTRIES)
        & (iota((ROWS, ROWS), 0) < GROUPS)
    ).astype(F32)

    def expand(rows):
        blocks = [jnp.where(grp_lane // 2 == grp, row, 0.0) for row in rows]
        wide = jnp.dot(
            jnp.concatenate(blocks, axis=0), spread_h, precision=HIGHEST, preferred_element_type=F32
        )
        return [wide[PAIRS * k : PAIRS * (k + 1)] for k in range(len(rows))]

    keep = lane < GROUPS
    ratio = jnp.concatenate([jnp.exp(mid - logs), jnp.exp(logs - mid)], axis=0)
    ratio = jnp.where(keep, ratio, 0.0)
    hi = ratio.astype(BF16)
    lo = ratio - hi.astype(F32)
    both = hi.astype(F32) + pltpu.roll(lo, GROUPS, 1)
    both = both.astype(BF16)
    mixed_v[...] = both

    def spread(part):
        for k in range(PAIRS // 2):
            src = iota((ROWS, 256), 0)
            dst = iota((ROWS, 256), 1) + 256 * k
            pick = ((src % GROUPS == dst // ENTRIES) & (src < 2 * GROUPS)).astype(F32).astype(BF16)
            wide = jnp.dot(
                mixed_v[ROWS * part : ROWS * (part + 1), :], pick, preferred_element_type=F32
            )
            expf_v[part, 2 * k] = wide[:, :ROWS]
            expf_v[part, 2 * k + 1] = wide[:, ROWS:]

    spread(0)

    ph = unit
    for b in range(8):
        bt_v[0, pl.ds(b, PAIRS, 8), :] = ph[0]
        bt_v[1, pl.ds(b, PAIRS, 8), :] = ph[1]
        mag = jnp.exp(-rate * float(b + 1))
        bt_v[2, pl.ds(b, PAIRS, 8), :] = mag
        bt_v[3, pl.ds(b, PAIRS, 8), :] = 1.0 / mag
        ph8 = ph
        ph = cmul(ph, unit)
    ph = (jnp.ones_like(cos1), jnp.zeros_like(cos1))
    for a in range(8, 16):
        at_v[0, a], at_v[1, a] = ph
        mag = jnp.exp(-rate * float(8 * (a - 8)))
        at_v[2, a], at_v[3, a] = mag, 1.0 / mag
        ph = cmul(ph, ph8)
        back = 16 - (a + 1)
        at_v[0, back], at_v[1, back] = ph[0], -ph[1]
        mag = jnp.exp(rate * float(8 * (8 - back)))
        at_v[2, back], at_v[3, back] = mag, 1.0 / mag

    def table(part, store):
        @pl.loop(0, PAIRS)
        def _(r):
            cb, sb, mb = (bt_v[k, pl.ds(r * 8, 8), :] for k in (0, 1, 3 - part))
            for a in range(16):
                ca, sa, ma = (
                    jnp.broadcast_to(at_v[k, a, pl.ds(r, 1), :], (8, ROWS)) for k in (0, 1, 3 - part)
                )
                c, s = cmul((ca, sa), (cb, sb))
                span = slice(8 * a, 8 * a + 8)
                store(r, span, c, s, ma * mb * expf_v[part, r, span, :])

    def backward(r, span, c, s, scale):
        wneg_v[0, r, span, :] = c * scale
        wneg_v[1, r, span, :] = -s * scale

    def forward(r, span, c, s, scale):
        wpos_v[0, r, span, :] = c * scale
        wpos_v[1, r, span, :] = s * scale

    table(0, backward)
    mid_wide, rest_wide = expand([mid, sigma - mid])
    p64 = power(64)
    end = cmul((at_v[0, 15], at_v[1, 15]), ph8)
    fall = jnp.exp(rest_wide) * jnp.exp(-rate * 64.0)
    last = (end[0] * fall, end[1] * fall)
    enter = (p64[0] * jnp.exp(mid_wide), p64[1] * jnp.exp(mid_wide))

    loads[7].wait()
    dec = expm1(-rate) * cos1 - 2.0 * jnp.sin(0.5 * theta) ** 2
    ims = jnp.exp(-rate) * sin1
    den = rate * rate + theta * theta
    zr = (ims * theta - dec * rate) / den
    zi = -(ims * rate + dec * theta) / den
    sum_v[0], sum_v[1] = zr, zi
    mask = iota((32, ROWS), 0) // 16 == iota((32, ROWS), 1) // ENTRIES
    for r in range(PAIRS):
        span = slice(32 * r, 32 * r + 32)
        br, bi = b_v[0, span, :], b_v[1, span, :]
        br = jnp.concatenate([br, br], axis=1)
        bi = jnp.concatenate([bi, bi], axis=1)
        wr, wi = cmul((sum_v[0, r : r + 1, :], sum_v[1, r : r + 1, :]), (br, bi))
        at = 32 * (r % 4)
        for k, w in enumerate((wr, wi)):
            lanes = slice(ROWS * k, ROWS * (k + 1))
            high, low = split(jnp.where(mask, w, 0.0))
            bw_v[r // 4, at : at + 32, lanes] = high
            bw_v[r // 4, ROWS + at : ROWS + at + 32, lanes] = low

    own_scaled, own_sq = half(tp)
    loads[2].wait()
    acc_v[...] = jnp.dot(
        own_scaled, win_v[pl.ds(tp * HALF, HALF), :], preferred_element_type=F32
    )

    if around:
        pl.semaphore_wait(ring2, len(around))
    sx[0]()
    for dev in far:
        pl.semaphore_signal(ring3, inc=1, device_id=dev)
    if nz > 2:
        pl.semaphore_wait(zring2, beside(1))
        tell(zring3, 2)

    tok_copy.wait_recv()
    gain_copy.wait_recv()
    far_scaled, far_sq = half(other)
    inv = lax.rsqrt((own_sq + far_sq) / D + 1e-06)
    loads[6].wait()
    acc = acc_v[...] + jnp.dot(
        far_scaled, win_v[pl.ds(other * HALF, HALF), :], preferred_element_type=F32
    )
    u_v[...] = (acc * inv).astype(BF16)

    quarter = iota((ROWS, ROWS), 1) // 32
    for j in range(4):
        uj = u_v[:, ROWS * j : ROWS * (j + 1)]
        stacked = jnp.concatenate(
            [jnp.where(quarter == i, uj, jnp.zeros_like(uj)) for i in range(4)], axis=0
        )
        drive = jnp.dot(
            jnp.concatenate([stacked, stacked], axis=1), bw_v[j], preferred_element_type=F32
        )
        for i in range(4):
            r = 4 * j + i
            d = drive[ROWS * i : ROWS * (i + 1)]
            q = cmul((wneg_v[0, r], wneg_v[1, r]), (d[:, :ROWS], d[:, ROWS:]))
            sum_v[0, r : r + 1, :] = jnp.sum(q[0], axis=0, keepdims=True)
            sum_v[1, r : r + 1, :] = jnp.sum(q[1], axis=0, keepdims=True)
            q_v[r, :, 0:ROWS] = q[0]
            q_v[r, :, ROWS:] = q[1]
    mine = cmul(last, (sum_v[0], sum_v[1]))

    def put(buf, index, value):
        buf[index, 0:PAIRS, :] = value[0]
        buf[index, PAIRS : 2 * PAIRS, :] = value[1]

    def take(buf, index):
        return (buf[index, 0:PAIRS, :], buf[index, PAIRS : 2 * PAIRS, :])

    put(mx_v, x, mine)
    mx[0]()

    spread(1)
    table(1, forward)
    def project(w):
        acc = jnp.dot(own_scaled, w[pl.ds(tp * HALF, HALF), :], preferred_element_type=F32)
        acc = acc + jnp.dot(far_scaled, w[pl.ds(other * HALF, HALF), :], preferred_element_type=F32)
        return (acc * inv).astype(BF16).astype(F32)

    loads[8].wait()
    loads[9].wait()
    pad_v[8:, :] = project(wc_v) * project(wv_v)
    if nz > 2:

        @pl.when(beside(2) > 0)
        def _():
            pl.semaphore_wait(zring3, beside(2))

    if nz > 4:

        @pl.when((z >= 4) & (z + 1 < nz))
        def _():
            pl.semaphore_signal(zring4, inc=1, device_id={"sz": z - 4})


    sx[1]()
    rows = [sx_v[k] for k in range(nx)]
    rho = functools.reduce(jnp.add, rows)
    sy_v[y] = rho
    if far:
        pl.semaphore_wait(ring3, len(far))
    sy[0]()
    index = (z * ny + y) * nx + x
    count = nz * ny * nx
    x1 = lax.rem(x + 1, nx)
    carry = x + 1 == nx
    y1 = jnp.where(carry, lax.rem(y + 1, ny), y)
    z1 = jnp.where(carry & (y + 1 == ny), lax.rem(z + 1, nz), z)
    tail_copy = pltpu.make_async_remote_copy(
        pad_v.at[ROWS : ROWS + 8],
        pad_v.at[0:8],
        tail_sem.at[0],
        tail_sem.at[1],
        device_id={"sz": z1, "sy": y1, "sx": x1},
    )
    pl.when(index + 1 < count)(tail_copy.start)

    wide = expand(rows)
    p128 = power(ROWS)
    ax = [(p128[0] * jnp.exp(w), p128[1] * jnp.exp(w)) for w in wide]

    def sweep(steps, values, start, here):
        total = before = start
        for k in range(len(steps)):
            if k:
                before = tuple(jnp.where(here == k, t, b) for t, b in zip(total, before))
            total = cmul(steps[k], total)
            if values is not None:
                total = cadd(total, values[k])
        return before, total

    one = (jnp.ones_like(cos1), jnp.zeros_like(cos1))
    zero = (jnp.zeros_like(cos1), jnp.zeros_like(cos1))
    dx, _ = sweep(ax, None, one, x)

    mx[1]()
    pre_x, row_total = sweep(ax, [take(mx_v, k) for k in range(nx)], zero, x)
    put(my_v, y, row_total)
    my[0]()

    loads[10].wait()
    for r in range(PAIRS):
        span = slice(32 * r, 32 * r + 32)
        cr, ci = c_v[0, span, :], c_v[1, span, :]
        cw_v[span, 0:ROWS] = jnp.where(mask, jnp.concatenate([cr, cr], axis=1), 0.0)
        cw_v[span, ROWS:] = jnp.where(mask, jnp.concatenate([ci, ci], axis=1), 0.0)
    tri16 = jnp.concatenate([tri.astype(BF16), tri.astype(BF16)], axis=1)
    sign = jnp.where(iota((1, 256), 1) < ROWS, 1.0, -1.0)
    nt = (((1,), (1,)), ((), ()))

    def gathered(wide):
        total = jnp.where(quarter == 0, wide[0:ROWS], 0.0)
        for i in range(1, 4):
            total = jnp.where(quarter == i, wide[ROWS * i : ROWS * (i + 1)], total)
        return total

    def read_out(high, low, weights):
        wide = lax.dot_general(high, weights, nt, preferred_element_type=F32)
        rest = lax.dot_general(low, weights[0:ROWS], nt, preferred_element_type=F32)
        return gathered(wide[:, :ROWS] + wide[:, ROWS:] + rest)

    loads[13].wait()
    for j in range(4):
        highs, lows = [], []
        for i in range(4):
            r = 4 * j + i
            pre = jnp.dot(
                tri16, jnp.concatenate(split(q_v[r]), axis=0), preferred_element_type=F32
            )
            st = cmul((wpos_v[0, r], wpos_v[1, r]), (pre[:, :ROWS], pre[:, ROWS:]))
            high, low = zip(*(split(part) for part in st))
            highs.append(jnp.concatenate(high, axis=1))
            lows.append(jnp.concatenate(low, axis=1))
            for k in range(2):
                lanes = slice(ROWS * k, ROWS * (k + 1))
                span = slice(ROWS * r, ROWS * (r + 1))
                wposb_v[0, span, lanes], wposb_v[1, span, lanes] = split(wpos_v[k, r])
        cols = slice(ROWS * j, ROWS * (j + 1))
        weights = jnp.concatenate(split(cw_v[cols, :] * sign), axis=0)
        read = read_out(jnp.concatenate(highs, axis=0), jnp.concatenate(lows, axis=0), weights)
        ypre_v[:, cols] = read + skip_v[:, cols] * u_v[:, cols].astype(F32)

    loads[11].wait()
    bg_v[...] = project(wb_v)

    @pl.when(index == 0)
    def _():
        pad_v[0:8, :] = jnp.zeros((8, CH), F32)

    pl.when(index > 0)(tail_copy.wait_recv)
    loads[15].wait()
    loads[16].wait()
    conv = pad_v[6 : 6 + ROWS, :] * taps_v[0:1, :]
    conv = conv + pad_v[7 : 7 + ROWS, :] * taps_v[1:2, :]
    conv = conv + pad_v[8 : 8 + ROWS, :] * taps_v[2:3, :]

    def head_norm(values, gain, width):
        same = iota((ROWS, ROWS), 0) // width == iota((ROWS, ROWS), 1) // width
        mean = jnp.where(same, 1.0 / width, 0.0).astype(BF16)
        mean = jnp.concatenate([mean, mean], axis=0)
        pieces = []
        for j in range(4):
            cols = slice(ROWS * j, ROWS * (j + 1))
            v = values[:, cols]
            m = jnp.dot(
                jnp.concatenate(split(v * v), axis=1), mean, preferred_element_type=F32
            )
            pieces.append((v * lax.rsqrt(m + 1e-06) * gain[:, cols]).astype(BF16))
        return jnp.concatenate(pieces, axis=1)

    conv_out = head_norm(bg_v[...] * conv, cgain_v[...], 64)
    loads[17].wait()
    for c in range(4):
        cpart_v[:, CH * c : CH * (c + 1)] = jnp.dot(
            conv_out, woc_v[:, CH * c : CH * (c + 1)], preferred_element_type=F32
        )

    sy[1]()
    rows = [sy_v[k] for k in range(ny)]
    pi = functools.reduce(jnp.add, rows)
    sz_v[z] = pi
    sz[0](1, 5)
    p512 = power(ROWS * nx)
    ay = [(p512[0] * jnp.exp(w), p512[1] * jnp.exp(w)) for w in expand(rows)]
    dy, _ = sweep(ay, None, one, y)
    pz = power(ROWS * nx * ny)

    my[1]()
    pre_y, plane_total = sweep(ay, [take(my_v, k) for k in range(ny)], zero, y)
    put(mz_v, z, plane_total)
    mz[0](1, 5)
    if nz > 4:

        @pl.when(z + 5 < nz)
        def _():
            pl.semaphore_wait(zring4, 1)

        sz[0](5, nz)
        mz[0](5, nz)

    sz[1]()
    az = [(pz[0] * jnp.exp(w), pz[1] * jnp.exp(w)) for w in expand([sz_v[k] for k in range(nz)])]
    loads[12].wait()
    start = (paired(init_v, (0,)), paired(init_v, (1,)))
    loads[14].wait()
    loads[18].wait()

    tok_copy.wait_send()
    gain_copy.wait_send()
    pl.when(index + 1 < count)(tail_copy.wait_send)
    for ex in (sx, mx, sy, my):
        ex[2]()

    mz[1]()
    pre_z, _ = sweep(az, [take(mz_v, k) for k in range(nz)], start, z)
    entry = cadd(cmul(dx, cadd(cmul(dy, pre_z), pre_y)), pre_x)
    entry = cmul(enter, entry)
    sum_v[0], sum_v[1] = entry
    for r in range(PAIRS):
        span = slice(32 * r, 32 * r + 32)
        ce = cmul(
            (sum_v[0, r : r + 1, :], sum_v[1, r : r + 1, :]), (cw_v[span, 0:ROWS], cw_v[span, ROWS:])
        )
        at = 32 * (r % 4)
        for k, w in enumerate((ce[0], -ce[1])):
            lanes = slice(ROWS * k, ROWS * (k + 1))
            high, low = split(w)
            ce_v[r // 4, at : at + 32, lanes] = high
            ce_v[r // 4, ROWS + at : ROWS + at + 32, lanes] = low
    acts = []
    for j in range(4):
        cols = slice(ROWS * j, ROWS * (j + 1))
        span = slice(4 * ROWS * j, 4 * ROWS * (j + 1))
        pre = ypre_v[:, cols] + read_out(wposb_v[0, span, :], wposb_v[1, span, :], ce_v[j])
        acts.append(0.5 * pre * (1.0 + lax.erf(pre * math.sqrt(0.5))))
    sout_v[...] = head_norm(jnp.concatenate(acts, axis=1), sgain_v[...], 16)

    sends = []
    for c in range(4):
        cols = slice(CH * c, CH * (c + 1))
        part = jnp.dot(sout_v[...], wos_v[:, cols], preferred_element_type=F32) + cpart_v[:, cols]
        part_v[c] = part.astype(BF16)
        send = pltpu.make_async_remote_copy(
            part_v.at[c, pl.ds(other * 64, 64)],
            got_v.at[c],
            part_ss.at[c],
            part_rs.at[c],
            device_id={"tp": other},
        )
        send.start()
        sends.append(send)
    sz[2]()
    mz[2]()
    for c in range(4):
        cols = slice(CH * c, CH * (c + 1))
        sends[c].wait_recv()
        own = part_v[c, pl.ds(tp * 64, 64), :].astype(F32)
        out[:, cols] = (own + got_v[c].astype(F32)).astype(BF16)
    for c in range(4):
        sends[c].wait_send()


def body(dims, *args):
    args = list(args)
    args[9] = jnp.swapaxes(args[9], 2, 3).reshape(2, CH, ENTRIES)
    args[10] = args[10].reshape(2, CH, ENTRIES)
    for k in (12, 13, 14):
        args[k] = args[k].reshape(1, CH)
    args = [pltpu.with_memory_space_constraint(a, pltpu.MemorySpace.HBM) for a in args]
    nz, ny, nx = dims
    anyspace = pl.BlockSpec(memory_space=pltpu.MemorySpace.HBM)
    vm = pltpu.VMEM
    dma = pltpu.SemaphoreType.DMA
    scratch = [
        vm((2, ROWS, HALF), BF16),
        vm((2, 1, HALF), BF16),
        vm((D, CH), BF16),
        vm((D, CH), BF16),
        vm((D, CH), BF16),
        vm((D, CH), BF16),
        vm((GROUPS, ENTRIES), F32),
        vm((GROUPS, ENTRIES), F32),
        vm((GROUPS, ROWS), F32),
        vm((2, CH, ENTRIES), F32),
        vm((2, CH, ENTRIES), F32),
        vm((2, GROUPS, ENTRIES), F32),
        vm((1, CH), F32),
        vm((1, CH), F32),
        vm((1, CH), F32),
        vm((3, CH), F32),
        vm((CH, D), BF16),
        vm((CH, D), BF16),
        vm((ROWS, CH), F32),
        vm((ROWS, CH), BF16),
        vm((4, 256, 256), BF16),
        vm((CH, 256), F32),
        vm((4, 256, 256), BF16),
        vm((2, PAIRS, ROWS, ROWS), F32),
        vm((4, 16, PAIRS, ROWS), F32),
        vm((4, ROWS, ROWS), F32),
        vm((2, PAIRS, ROWS, ROWS), F32),
        vm((2, PAIRS, ROWS, ROWS), F32),
        vm((2, PAIRS * ROWS, 256), BF16),
        vm((PAIRS, ROWS, 256), F32),
        vm((2, PAIRS, ROWS), F32),
        vm((256, ROWS), BF16),
        vm((ROWS, CH), F32),
        vm((ROWS + 8, CH), F32),
        vm((ROWS, CH), F32),
        vm((ROWS, D), F32),
        vm((ROWS, CH), BF16),
        vm((4, ROWS, CH), BF16),
        vm((4, 64, CH), BF16),
        vm((nx, 1, ROWS), F32),
        vm((ny, 1, ROWS), F32),
        vm((nz, 1, ROWS), F32),
        vm((nx, 32, ROWS), F32),
        vm((ny, 32, ROWS), F32),
        vm((nz, 32, ROWS), F32),
        dma((19,)),
        dma((4,)),
        dma((2,)),
        dma((4,)),
        dma((4,)),
        dma((2, nx)),
        dma((2, ny)),
        dma((2, nz)),
        dma((2, nx)),
        dma((2, ny)),
        dma((2, nz)),
        *[pltpu.SemaphoreType.REGULAR] * 5,
    ]
    return pl.pallas_call(
        functools.partial(kernel, dims),
        out_shape=jax.ShapeDtypeStruct((64, D), BF16),
        in_specs=[anyspace] * len(args),
        out_specs=pl.BlockSpec(memory_space=pltpu.MemorySpace.VMEM),
        scratch_shapes=scratch,
        compiler_params=pltpu.CompilerParams(
            collective_id=0, has_side_effects=True, vmem_limit_bytes=48 * 1024 * 1024
        ),
        name="layer",
    )(*args)


def solution(mesh):
    dims = SP_DIMS
    finer = Mesh(mesh.devices.reshape(*dims, mesh.shape["tp"]), (*SP, "tp"))
    placed = (
        P(SP, "tp"),
        P(None, "tp"),
        P(None, "tp"),
        P(None, "tp"),
        P(None, "tp"),
        P(None, "tp"),
        P("tp", None),
        P("tp", None),
        P("tp", SP),
        P(None, "tp", None, None),
        P(None, "tp", None, None),
        P(None, "tp", None),
        P("tp"),
        P("tp"),
        P("tp"),
        P(None, "tp"),
        P("tp", None),
        P("tp", None),
    )
    return jax.shard_map(
        functools.partial(body, dims),
        mesh=finer,
        in_specs=placed,
        out_specs=P((*SP, "tp"), None),
        check_vma=False,
    )
```
